256 devices in a mesh: grp: 2 (over z), ep: 64 (over y, x), tp: 2 (over core).
Axes of the slice: x: 8, y: 8, z: 2, core: 2. Of those that a mesh axis runs over, the one named last changes fastest.
The devices are a block of a 8x8x16 slice.
Arguments:
- hidden_in: bfloat16 [2048, 2048], P(('grp', 'ep', 'tp')), parts along dimension 0, may hold values from -6 to 6
- query_nope: bfloat16 [2048, 16, 64], P(('grp', 'ep', 'tp')), parts along dimension 0, may hold values from -102 to 102
- query_rope: bfloat16 [2048, 16, 32], P(('grp', 'ep', 'tp')), parts along dimension 0, may hold values from -6 to 6
- new_latent: bfloat16 [2048, 256], P(('grp', 'ep', 'tp')), parts along dimension 0, may hold values from -6 to 6
- new_rope: bfloat16 [2048, 32], P(('grp', 'ep', 'tp')), parts along dimension 0, may hold values from -6 to 6
- cache_latent: bfloat16 [2048, 1024, 256], P(('grp', 'ep', 'tp')), parts along dimension 0, may hold values from -6 to 6
- cache_rope: bfloat16 [2048, 1024, 32], P(('grp', 'ep', 'tp')), parts along dimension 0, may hold values from -6 to 6
- lengths: int32 [2048], P(('grp', 'ep', 'tp')), parts along dimension 0, may hold values from 1 to 1024, as said below
- absorb_key: bfloat16 [256, 16, 64], replicated, may hold values from -0.75 to 0.75
- value_up: bfloat16 [256, 16, 128], replicated, may hold values from -0.375 to 0.375
- out_proj: bfloat16 [2048, 2048], P(None, ('ep', 'tp')), may hold values from -0.125 to 0.125
- gain_mix: bfloat16 [2048], replicated, may hold values from 0.099609375 to 1.8984375
- gain_ffn_in: bfloat16 [2048], replicated, may hold values from 0.099609375 to 1.8984375
- router: bfloat16 [2048, 128], replicated, may hold values from -0.125 to 0.125
- routes: int32 [2048, 6], P(('grp', 'ep')), parts along dimension 0, may hold values from 0 to 127, all different within a row; in each aligned block of 16 rows (0 to 15, 16 to 31, ...) at most 2 rows name the same one
- expert_gate: bfloat16 [128, 2048, 256], P(('ep', 'tp')), may hold values from -0.125 to 0.125
- expert_up: bfloat16 [128, 2048, 256], P(('ep', 'tp')), may hold values from -0.125 to 0.125
- expert_down: bfloat16 [128, 256, 2048], P(('ep', 'tp')), may hold values from -0.375 to 0.375
- shared_gate: bfloat16 [2048, 256], replicated, may hold values from -0.125 to 0.125
- shared_up: bfloat16 [2048, 256], replicated, may hold values from -0.125 to 0.125
- shared_down: bfloat16 [256, 2048], replicated, may hold values from -0.375 to 0.375
- gain_ffn_out: bfloat16 [2048], replicated, may hold values from 0.099609375 to 1.8984375
Outputs:
- layer_out: bfloat16 [2048, 2048], P(('grp', 'ep', 'tp')), parts along dimension 0
The draws below stay inside these ranges and needn't reach their ends.
There are 2 independent parts, one for each index of `grp`. The reference program is written for one: setup_inputs(seed, part) draws one part's arguments, and reference() takes and returns one part's arrays. A program takes and returns all parts, laid end to end along the dimension named above; an argument that names none is the same for every part. Nothing has to cross between parts.
Inputs may be any that keep to these rules, and one draw needn't show every extreme that they name: `lengths`: every sequence holds 1 to 1024 cached positions, and some sequence holds 1024. `routes`: each row names 6 different experts; in each aligned block of 16 rows (the rows of one index of ep) no expert is named by more than 2 rows, and in some block some expert is named by exactly 2 rows.
All inputs are finite; a program needn't handle non-finite values.
Results may differ from the reference program's by a relative error of at most 0.015.
Values may be sent and summed in bfloat16 or wider, within the bound.
No kernel may reach another device: no remote copies, remote signals or barrier semaphores. Data moves between devices by JAX's collectives and lax.ppermute only.
A program may use at most 64 MiB of HBM per device.

```python
import math
import jax
import jax.numpy as jnp
import numpy as np
from jax import lax

D = 2048
HEADS = 16
NOPE = 64
ROPE = 32
VHEAD = 128
LAT = 256
FE = 256
FS = 256
TOPK = 6
CTX = 1024
SEQ_DEV = 8
NSEQ = 1024
TOK_GROUP = 16
EXPERTS = 128
CAP = 2
N_EP = 64


def draw_query_nope(key, part):
    base_key = jax.random.fold_in(jax.random.fold_in(key, 23), 0)
    values = jnp.clip(jax.random.normal(base_key, (NSEQ, HEADS, NOPE), jnp.float32), -6.0, 6.0)
    return values.astype(jnp.bfloat16)


def draw_lengths(key, part):
    level_key, value_key, pick_key = jax.random.split(jax.random.fold_in(key, 11), 3)
    device_count = NSEQ // SEQ_DEV
    level_draw = jax.random.randint(level_key, (device_count,), 1, 5)
    length_limit = jnp.maximum(jnp.repeat(level_draw * level_draw * CTX // 16, SEQ_DEV), 1)
    raw_draw = jax.random.randint(value_key, (NSEQ,), 0, 1 << 20)
    drawn_lengths = 1 + raw_draw % length_limit
    chosen_row = jax.random.randint(pick_key, (), 0, NSEQ)
    drawn_lengths = jnp.where(jnp.arange(NSEQ) == chosen_row, CTX, drawn_lengths)
    return drawn_lengths.astype(jnp.int32)


def steps_of(stream_key, shape, pieces, low, high):
    def one(axis_at, shards_of):
        draws = jax.random.uniform(jax.random.fold_in(jax.random.fold_in(stream_key, 6), axis_at), (shards_of,), jnp.float32, low / len(pieces), high / len(pieces))
        return jnp.repeat(jnp.exp(draws), shape[axis_at] // shards_of).reshape((-1,) + (1,) * (len(shape) - axis_at - 1))

    gain = one(*pieces[0])
    for cut in pieces[1:]:
        gain = gain * one(*cut)
    return gain


def routed_block(own_key, own, number, rows, count, top, limit, slope):
    order = jax.random.permutation(own_key, count)
    crowded, usual = shares(count, rows * top, limit, slope, True), shares(count, rows * top, limit, slope, False)
    places = jnp.arange(count)

    def named(sizes, offset_by):
        used = int((sizes > 0).sum())
        fixed = max(1, used // 4)
        shifted = fixed + (places - fixed + offset_by * (used - fixed)) % max(1, count - fixed)
        return jnp.zeros((count,), jnp.int32).at[order[jnp.where(places < fixed, places, shifted)]].set(jnp.asarray(sizes, jnp.int32))

    sizes = jnp.where(number % 4 == 0, named(crowded, number // 4), named(usual, number - number // 4 - 1))
    mixed = jax.random.permutation(jax.random.fold_in(own, 3), count)
    giver, sink = mixed[0:count // 2 * 2:2], mixed[1:count // 2 * 2:2]
    margin = jnp.minimum(sizes[giver] - 1, limit - sizes[sink]) // 2
    margin = jnp.where((giver == order[0]) | (sink == order[0]) | (sizes[sink] == 0), 0, jnp.maximum(margin, 0))
    shifted = jax.random.randint(jax.random.fold_in(own, 4), (count // 2,), 0, 1 << 20) % (margin + 1)
    sizes = sizes.at[giver].add(-shifted).at[sink].add(shifted)
    items = jnp.searchsorted(jnp.cumsum(sizes), jnp.arange(rows * top), side="right").astype(jnp.int32)
    grid = items.reshape(top, rows).T
    grid = grid[jax.random.permutation(jax.random.fold_in(own, 1), rows)]
    offset_by = jax.random.randint(jax.random.fold_in(own, 2), (rows, 1), 0, top)
    return jnp.take_along_axis(grid, (jnp.arange(top)[None, :] + offset_by) % top, axis=1)


def shares(count, total, limit, lean, full):
    loads = [(1 << 20) // math.isqrt(rank ** lean) + 1 for rank in range(1, count + 1)]
    largest = limit if full else min(limit, max(-(-total // count), total * loads[0] // sum(loads)))
    least = 1 if total - largest >= count - 1 else 0
    counts, surplus = [largest] + [least] * (count - 1), total - largest - least * (count - 1)
    while surplus > 0:
        candidates = [i for i in range(1, count) if counts[i] < largest] or [i for i in range(1, count) if counts[i] < limit]
        whole, budget = sum([loads[i] for i in candidates]), surplus
        for i in candidates:
            addition = min(limit - counts[i], max(1, budget * loads[i] // whole), surplus)
            counts[i] = counts[i] + addition
            surplus = surplus - addition
    return np.array(counts)


def bell_draw(rng, shape, width, reach, pieces=(), kind=jnp.bfloat16):
    drawn = jax.random.normal(rng, shape, jnp.float32) * width
    if len(pieces) > 0:
        drawn = steps_of(rng, shape, pieces, -0.22, 0.18) * drawn
    return jnp.clip(drawn, min=-reach, max=reach).astype(kind)


def setup_inputs(seed: int = 0, part: int = 0) -> dict:
    key_of = jax.random.split(jax.random.key(seed), 23)
    own_keys = jax.random.split(jax.random.fold_in(key_of[22], part), 23)
    hidden_in = bell_draw(own_keys[0], (NSEQ, D), 1.0, 6.0, ((0, 128),))
    query_nope = draw_query_nope(jax.random.fold_in(jax.random.fold_in(key_of[22], part), 71), part)
    query_rope = bell_draw(own_keys[2], (NSEQ, HEADS, ROPE), 1.0, 6.0, ((0, 128),))
    new_latent = bell_draw(own_keys[3], (NSEQ, LAT), 1.0, 6.0, ((0, 128),))
    new_rope = bell_draw(own_keys[4], (NSEQ, ROPE), 1.0, 6.0, ((0, 128),))
    cache_latent = bell_draw(own_keys[5], (NSEQ, CTX, LAT), 1.0, 6.0, ((0, 128),))
    cache_rope = bell_draw(own_keys[6], (NSEQ, CTX, ROPE), 1.0, 6.0, ((0, 128),))
    lengths = draw_lengths(jax.random.fold_in(jax.random.fold_in(key_of[22], part), 71), part)
    absorb_key = bell_draw(key_of[8], (LAT, HEADS, NOPE), NOPE ** -0.5, 0.75)
    value_up = bell_draw(key_of[9], (LAT, HEADS, VHEAD), LAT ** -0.5, 0.375)
    out_proj = bell_draw(key_of[10], (HEADS * VHEAD, D), (HEADS * VHEAD) ** -0.5, 0.125, ((1, 128),))
    gain_mix = jnp.clip(1.0 + 0.18 * jax.random.normal(key_of[11], (D,), jnp.float32), 0.099609375, 1.8984375).astype(jnp.bfloat16)
    gain_ffn_in = jnp.clip(1.0 + 0.18 * jax.random.normal(key_of[12], (D,), jnp.float32), 0.099609375, 1.8984375).astype(jnp.bfloat16)
    router = bell_draw(key_of[13], (D, EXPERTS), D ** -0.5, 0.125)
    routes_keys = jax.random.split(jax.random.fold_in(own_keys[14], 1), NSEQ // TOK_GROUP)
    routes_turns = jax.random.permutation(jax.random.fold_in(own_keys[14], 3), NSEQ // TOK_GROUP)
    routes = jax.vmap(lambda own, number: routed_block(jax.random.fold_in(own_keys[14], 2), own, number, TOK_GROUP, EXPERTS, TOPK, CAP, 2))(routes_keys, routes_turns).reshape((NSEQ, TOPK))
    expert_gate = bell_draw(key_of[15], (EXPERTS, D, FE), D ** -0.5, 0.125, ((0, 128),))
    expert_up = bell_draw(key_of[16], (EXPERTS, D, FE), D ** -0.5, 0.125, ((0, 128),))
    expert_down = bell_draw(key_of[17], (EXPERTS, FE, D), FE ** -0.5, 0.375, ((0, 128),))
    shared_gate = bell_draw(key_of[18], (D, FS), D ** -0.5, 0.125)
    shared_up = bell_draw(key_of[19], (D, FS), D ** -0.5, 0.125)
    shared_down = bell_draw(key_of[20], (FS, D), FS ** -0.5, 0.375)
    gain_ffn_out = jnp.clip(1.0 + 0.18 * jax.random.normal(key_of[21], (D,), jnp.float32), 0.099609375, 1.8984375).astype(jnp.bfloat16)
    return dict(hidden_in=hidden_in, query_nope=query_nope, query_rope=query_rope, new_latent=new_latent, new_rope=new_rope, cache_latent=cache_latent, cache_rope=cache_rope, lengths=lengths, absorb_key=absorb_key, value_up=value_up, out_proj=out_proj, gain_mix=gain_mix, gain_ffn_in=gain_ffn_in, router=router, routes=routes, expert_gate=expert_gate, expert_up=expert_up, expert_down=expert_down, shared_gate=shared_gate, shared_up=shared_up, shared_down=shared_down, gain_ffn_out=gain_ffn_out)


rope_theta = 10000.0
norm_eps = 1e-06
routed_scale = 2.5
masked_score = -1e+30

def normalize(values):
    return values * lax.rsqrt(lax.optimization_barrier(jnp.mean(values * values, axis=-1, keepdims=True)) + norm_eps)

def rotate(values, positions):
    half_dim = values.shape[-1] // 2
    inverse = rope_theta ** (-jnp.arange(half_dim, dtype=jnp.float32) * 2.0 / values.shape[-1])
    angles = positions * inverse
    cosine = jnp.cos(angles)
    sine_table = jnp.sin(angles)
    first_half = values[..., :half_dim]
    second_half = values[..., half_dim:]
    return jnp.concatenate([first_half * cosine - second_half * sine_table, first_half * sine_table + second_half * cosine], axis=-1)

def swiglu(flat_rows, gate_w, up_w, down_w):
    gate_part = jnp.dot(flat_rows, gate_w, preferred_element_type=jnp.float32)
    up_part = jnp.dot(flat_rows, up_w, preferred_element_type=jnp.float32)
    inner_rows = (jax.nn.silu(gate_part) * up_part).astype(jnp.bfloat16)
    return jnp.dot(inner_rows, down_w, preferred_element_type=jnp.float32).astype(jnp.bfloat16)

def attend_group(group_args):
    query_latent, query_pe, latent_block, rope_block, latent_new, key_new, group_lengths = group_args
    score_scale = (NOPE + ROPE) ** (-0.5)
    cache_scores = (jnp.einsum('shc,skc->shk', query_latent.astype(jnp.float32), latent_block.astype(jnp.float32)) + jnp.einsum('shr,skr->shk', query_pe.astype(jnp.float32), rope_block.astype(jnp.float32))) * score_scale
    new_score = (jnp.einsum('shc,sc->sh', query_latent.astype(jnp.float32), latent_new.astype(jnp.float32)) + jnp.einsum('shr,sr->sh', query_pe.astype(jnp.float32), key_new.astype(jnp.float32))) * score_scale
    in_range = jnp.arange(CTX, dtype=jnp.int32)[None, None, :] < group_lengths[:, None, None]
    cache_scores = jnp.where(in_range, cache_scores, masked_score)
    row_max = jnp.maximum(lax.optimization_barrier(jnp.max(cache_scores, axis=-1)), new_score)
    cache_exp = jnp.exp(cache_scores - row_max[..., None])
    new_exp = jnp.exp(new_score - row_max)
    weight_total = lax.optimization_barrier(jnp.sum(cache_exp, axis=-1)) + new_exp
    cache_weights = lax.optimization_barrier(cache_exp.astype(jnp.bfloat16)).astype(jnp.float32)
    new_weight = lax.optimization_barrier(new_exp.astype(jnp.bfloat16)).astype(jnp.float32)
    weighted = jnp.einsum('shk,skc->shc', cache_weights, latent_block.astype(jnp.float32)) + new_weight[..., None] * latent_new.astype(jnp.float32)[:, None, :]
    return (weighted / weight_total[..., None]).astype(jnp.bfloat16)

def expert_apply(expert_args):
    flat_rows, gate_w, up_w, down_w = expert_args
    return swiglu(flat_rows, gate_w, up_w, down_w)

def reference(hidden_in, query_nope, query_rope, new_latent, new_rope, cache_latent, cache_rope, lengths, absorb_key, value_up, out_proj, gain_mix, gain_ffn_in, router, routes, expert_gate, expert_up, expert_down, shared_gate, shared_up, shared_down, gain_ffn_out):
    seq_count = hidden_in.shape[0]
    group_count = seq_count // SEQ_DEV
    positions = lengths.astype(jnp.float32)
    query_latent = jnp.einsum('shn,chn->shc', query_nope.astype(jnp.float32), absorb_key.astype(jnp.float32)).astype(jnp.bfloat16)
    query_pe = rotate(query_rope.astype(jnp.float32), positions[:, None, None]).astype(jnp.bfloat16)
    latent_new = normalize(new_latent.astype(jnp.float32)).astype(jnp.bfloat16)
    key_new = rotate(new_rope.astype(jnp.float32), positions[:, None]).astype(jnp.bfloat16)

    def grouped(values):
        return values.reshape((group_count, SEQ_DEV) + values.shape[1:])
    latent_out = lax.map(attend_group, (grouped(query_latent), grouped(query_pe), grouped(cache_latent), grouped(cache_rope), grouped(latent_new), grouped(key_new), grouped(lengths)))
    latent_out = latent_out.reshape(seq_count, HEADS, LAT)
    heads_out = jnp.einsum('shc,chv->shv', latent_out.astype(jnp.float32), value_up.astype(jnp.float32)).astype(jnp.bfloat16).reshape(seq_count, HEADS * VHEAD)
    mixed_rows = jnp.dot(heads_out, out_proj, preferred_element_type=jnp.float32).astype(jnp.bfloat16)
    after_mix = (hidden_in.astype(jnp.float32) + gain_mix.astype(jnp.float32) * normalize(mixed_rows.astype(jnp.float32))).astype(jnp.bfloat16)
    ffn_in = (normalize(after_mix.astype(jnp.float32)) * gain_ffn_in.astype(jnp.float32)).astype(jnp.bfloat16)
    affinity = jax.nn.sigmoid(jnp.dot(ffn_in, router, preferred_element_type=jnp.float32))
    chosen = jnp.take_along_axis(affinity, routes, axis=1)
    route_weights = chosen / lax.optimization_barrier(jnp.sum(chosen, axis=-1, keepdims=True)) * routed_scale
    pair_count = TOK_GROUP * TOPK
    expert_ids = routes.reshape(N_EP, pair_count)
    order_index = jnp.arange(pair_count, dtype=jnp.int32)
    same_expert = expert_ids[:, :, None] == expert_ids[:, None, :]
    earlier = order_index[None, :] < order_index[:, None]
    slot_number = lax.optimization_barrier(jnp.sum(jnp.logical_and(same_expert, earlier[None]), axis=2)).astype(jnp.int32)
    slot_number = slot_number.reshape(seq_count, TOPK)
    group_index = (jnp.arange(seq_count, dtype=jnp.int32) // TOK_GROUP)[:, None]
    slot_index = (routes * (N_EP * CAP) + group_index * CAP + slot_number).astype(jnp.int32)
    buffer = jnp.zeros((EXPERTS * N_EP * CAP, D), jnp.bfloat16)
    buffer = buffer.at[slot_index.reshape(-1)].set(jnp.repeat(ffn_in, TOPK, axis=0))
    outputs = lax.map(expert_apply, (buffer.reshape(EXPERTS, N_EP * CAP, D), expert_gate, expert_up, expert_down))
    picked = outputs.reshape(EXPERTS * N_EP * CAP, D)[slot_index]
    routed = lax.optimization_barrier(jnp.sum(picked.astype(jnp.float32) * route_weights[..., None], axis=1))
    shared = swiglu(ffn_in, shared_gate, shared_up, shared_down)
    combined = routed + shared.astype(jnp.float32)
    return (after_mix.astype(jnp.float32) + gain_ffn_out.astype(jnp.float32) * normalize(combined)).astype(jnp.bfloat16)
```

```python
import jax
import jax.numpy as jnp
from jax import lax
from jax.sharding import Mesh
from jax.sharding import PartitionSpec as P

ABLK = 512
EP = ("ep_0", "ep_1")
GRP_EP_TP = ("grp", "ep_0", "ep_1", "tp")
EP_TP = ("ep_0", "ep_1", "tp")
GRP_EP = ("grp", "ep_0", "ep_1")


rope_theta = 10000.0
norm_eps = 1e-06
routed_scale = 2.5
masked_score = -1e30


def device_at(row, col, core):
    return (row * 8 + col) * 2 + core


BLOCKS = [
    [
        device_at(2 * block_row + i, 2 * block_col + j, core)
        for i in range(2)
        for j in range(2)
        for core in range(2)
    ]
    for block_row in range(4)
    for block_col in range(4)
]
PLACES = [list(members) for members in zip(*BLOCKS)]


def exchanged(blocks, groups):
    return lax.all_to_all(blocks, EP_TP, 0, 0, axis_index_groups=groups, tiled=True)


def sent_to_all(array, groups):
    count = len(groups[0])
    return exchanged(jnp.broadcast_to(array[None], (count, *array.shape)), groups)


def from_other_core(array):
    return lax.ppermute(array, "tp", [(0, 1), (1, 0)])


def normalize(values):
    return values * lax.rsqrt(jnp.mean(values * values, axis=-1, keepdims=True) + norm_eps)


def rotate(values, positions):
    half_dim = values.shape[-1] // 2
    inverse = rope_theta ** (-jnp.arange(half_dim, dtype=jnp.float32) * 2.0 / values.shape[-1])
    angles = positions * inverse
    cosine = jnp.cos(angles)
    sine_table = jnp.sin(angles)
    first_half = values[..., :half_dim]
    second_half = values[..., half_dim:]
    return jnp.concatenate(
        [
            first_half * cosine - second_half * sine_table,
            first_half * sine_table + second_half * cosine,
        ],
        axis=-1,
    )


def swiglu(flat_rows, gate_w, up_w, down_w):
    gate_part = jnp.dot(flat_rows, gate_w, preferred_element_type=jnp.float32)
    up_part = jnp.dot(flat_rows, up_w, preferred_element_type=jnp.float32)
    inner_rows = (jax.nn.silu(gate_part) * up_part).astype(jnp.bfloat16)
    return jnp.dot(inner_rows, down_w, preferred_element_type=jnp.float32).astype(jnp.bfloat16)


def attention(
    query_nope,
    query_rope,
    new_latent,
    new_rope,
    cache_latent,
    cache_rope,
    lengths,
    absorb_key,
    value_up,
):
    seq_count = query_nope.shape[0]
    positions = lengths.astype(jnp.float32)
    query_latent = jnp.einsum(
        "shn,chn->shc", query_nope, absorb_key, preferred_element_type=jnp.float32
    ).astype(jnp.bfloat16)
    query_pe = rotate(query_rope.astype(jnp.float32), positions[:, None, None]).astype(jnp.bfloat16)
    latent_new = normalize(new_latent.astype(jnp.float32)).astype(jnp.bfloat16)
    key_new = rotate(new_rope.astype(jnp.float32), positions[:, None]).astype(jnp.bfloat16)
    score_scale = (query_nope.shape[-1] + query_rope.shape[-1]) ** (-0.5)
    new_score = (
        jnp.einsum("shc,sc->sh", query_latent, latent_new, preferred_element_type=jnp.float32)
        + jnp.einsum("shr,sr->sh", query_pe, key_new, preferred_element_type=jnp.float32)
    ) * score_scale

    def attend_block(block_index, loop_state):
        running_max, weight_total, weighted_sum = loop_state
        block_start = block_index * ABLK
        block_latent = lax.dynamic_slice_in_dim(cache_latent, block_start, ABLK, 1)
        block_rope = lax.dynamic_slice_in_dim(cache_rope, block_start, ABLK, 1)
        scores = (
            jnp.einsum(
                "shc,skc->shk", query_latent, block_latent, preferred_element_type=jnp.float32
            )
            + jnp.einsum("shr,skr->shk", query_pe, block_rope, preferred_element_type=jnp.float32)
        ) * score_scale
        key_index = block_start + lax.iota(jnp.int32, ABLK)
        in_range = key_index[None, None, :] < lengths[:, None, None]
        scores = jnp.where(in_range, scores, masked_score)
        new_max = jnp.maximum(running_max, jnp.max(scores, axis=-1))
        rescale = jnp.exp(running_max - new_max)
        weights = jnp.exp(scores - new_max[..., None])
        weight_total = weight_total * rescale + jnp.sum(weights, axis=-1)
        weighted_sum = weighted_sum * rescale[..., None] + jnp.einsum(
            "shk,skc->shc",
            weights.astype(jnp.bfloat16),
            block_latent,
            preferred_element_type=jnp.float32,
        )
        return (new_max, weight_total, weighted_sum)

    longest = jnp.max(lengths)
    block_count = (longest + ABLK - 1) // ABLK
    ones_start = jnp.ones_like(new_score)
    sum_start = ones_start[..., None] * latent_new.astype(jnp.float32)[:, None, :]
    final_max, weight_total, weighted_sum = lax.fori_loop(
        0, block_count, attend_block, (new_score, ones_start, sum_start)
    )
    latent_out = (weighted_sum / weight_total[..., None]).astype(jnp.bfloat16)
    return (
        jnp.einsum("shc,chv->shv", latent_out, value_up, preferred_element_type=jnp.float32)
        .astype(jnp.bfloat16)
        .reshape(seq_count, -1)
    )


def in_column_order(pieces):
    count, width = pieces.shape[1], pieces.shape[0] * pieces.shape[2]
    split = pieces.reshape(2, 2, 2, count, 4, 4, pieces.shape[2] // 16)
    return split.transpose(3, 4, 0, 5, 1, 2, 6).reshape(count, width)


def local(
    hidden_in,
    query_nope,
    query_rope,
    new_latent,
    new_rope,
    cache_latent,
    cache_rope,
    lengths,
    absorb_key,
    value_up,
    out_proj,
    gain_mix,
    gain_ffn_in,
    router,
    routes,
    expert_gate,
    expert_up,
    expert_down,
    shared_gate,
    shared_up,
    shared_down,
    gain_ffn_out,
):
    seq_count, width = hidden_in.shape
    core = lax.axis_index("tp")
    own_start = core * seq_count
    slab = sent_to_all(out_proj.T, PLACES).reshape(-1, out_proj.shape[0])
    chip_hidden = lax.all_gather(hidden_in, "tp", axis=0, tiled=True)
    heads_out = attention(
        query_nope,
        query_rope,
        new_latent,
        new_rope,
        cache_latent,
        cache_rope,
        lengths,
        absorb_key,
        value_up,
    )
    block_heads = sent_to_all(heads_out, BLOCKS).reshape(-1, heads_out.shape[1])
    partial = lax.dot_general(
        block_heads, slab, (((1,), (1,)), ((), ())), preferred_element_type=jnp.float32
    ).astype(jnp.bfloat16)
    chip_rows = partial.reshape(len(BLOCKS[0]) // 2, 1, 2 * seq_count, -1)
    chip_rows = jnp.broadcast_to(chip_rows, (chip_rows.shape[0], 2, *chip_rows.shape[2:]))
    pieces = exchanged(chip_rows.reshape(len(BLOCKS[0]), *chip_rows.shape[2:]), BLOCKS)
    mixed = in_column_order(pieces)
    after_mix = (
        chip_hidden.astype(jnp.float32)
        + gain_mix.astype(jnp.float32) * normalize(mixed.astype(jnp.float32))
    ).astype(jnp.bfloat16)
    ffn_in = (normalize(after_mix.astype(jnp.float32)) * gain_ffn_in.astype(jnp.float32)).astype(
        jnp.bfloat16
    )
    experts_total = router.shape[1]
    group_rows, top_count = routes.shape
    ep_count = lax.axis_size(EP)
    capacity = 2 * ((group_rows * top_count + experts_total - 1) // experts_total)
    slots = ep_count * capacity
    slot_index = lax.iota(jnp.int32, slots)
    slot_expert = (slot_index // capacity) * 2 + core
    named = jnp.any(routes[:, :, None] == slot_expert[None, None, :], axis=1)
    earlier = jnp.tril(jnp.ones((group_rows, group_rows), jnp.bfloat16), -1)
    before = jnp.dot(earlier, named.astype(jnp.bfloat16), preferred_element_type=jnp.float32)
    taken = jnp.logical_and(named, before == (slot_index % capacity).astype(jnp.float32)[None, :])
    outgoing = lax.dot_general(
        taken.astype(jnp.bfloat16),
        ffn_in,
        (((0,), (0,)), ((), ())),
        preferred_element_type=jnp.float32,
    ).astype(jnp.bfloat16)
    received = lax.all_to_all(
        outgoing.reshape(ep_count, capacity, width), EP, split_axis=0, concat_axis=0, tiled=True
    )
    affinity = jax.nn.sigmoid(jnp.dot(ffn_in, router, preferred_element_type=jnp.float32))
    choose = routes[..., None] == lax.iota(jnp.int32, experts_total)[None, None, :]
    chosen = jnp.sum(jnp.where(choose, affinity[:, None, :], 0.0), axis=-1)
    route_weights = chosen / jnp.sum(chosen, axis=-1, keepdims=True) * routed_scale
    slot_weights = jnp.sum(
        jnp.where(
            routes[:, :, None] == slot_expert[None, None, :], route_weights[:, :, None], 0.0
        ),
        axis=1,
    )
    slot_weights = jnp.where(taken, slot_weights, 0.0)
    weights_high = slot_weights.astype(jnp.bfloat16)
    weights_low = (slot_weights - weights_high.astype(jnp.float32)).astype(jnp.bfloat16)
    own_ffn = lax.dynamic_slice_in_dim(ffn_in, own_start, seq_count, 0)
    own_mix = lax.dynamic_slice_in_dim(after_mix, own_start, seq_count, 0)
    shared = swiglu(own_ffn, shared_gate, shared_up, shared_down)
    outputs = swiglu(
        received.reshape(slots, width), expert_gate[0], expert_up[0], expert_down[0]
    )
    returned = lax.all_to_all(
        outputs.reshape(ep_count, capacity, width), EP, split_axis=0, concat_axis=0, tiled=True
    ).reshape(slots, width)
    both = jnp.dot(
        jnp.concatenate([weights_high, weights_low], axis=0),
        returned,
        preferred_element_type=jnp.float32,
    )
    routed = both[:group_rows] + both[group_rows:]
    kept = lax.dynamic_slice_in_dim(routed, own_start, seq_count, 0)
    given = lax.dynamic_slice_in_dim(routed, seq_count - own_start, seq_count, 0)
    combined = kept + from_other_core(given) + shared.astype(jnp.float32)
    return (
        own_mix.astype(jnp.float32) + gain_ffn_out.astype(jnp.float32) * normalize(combined)
    ).astype(jnp.bfloat16)


def solution(mesh):
    torus = Mesh(
        mesh.devices.reshape(mesh.shape["grp"], 8, 8, mesh.shape["tp"]),
        ("grp", "ep_0", "ep_1", "tp"),
    )
    in_specs = (
        P(GRP_EP_TP, None),
        P(GRP_EP_TP, None, None),
        P(GRP_EP_TP, None, None),
        P(GRP_EP_TP, None),
        P(GRP_EP_TP, None),
        P(GRP_EP_TP, None, None),
        P(GRP_EP_TP, None, None),
        P(GRP_EP_TP),
        P(),
        P(),
        P(None, EP_TP),
        P(),
        P(),
        P(),
        P(GRP_EP, None),
        P(EP_TP, None, None),
        P(EP_TP, None, None),
        P(EP_TP, None, None),
        P(),
        P(),
        P(),
        P(),
    )
    out_specs = P(GRP_EP_TP, None)
    return jax.shard_map(local, mesh=torus, in_specs=in_specs, out_specs=out_specs, check_vma=False)
```

```python
import jax
import jax.numpy as jnp
from jax import lax
from jax.experimental import pallas as pl
from jax.experimental.pallas import tpu as pltpu
from jax.sharding import Mesh
from jax.sharding import PartitionSpec as P

SEQ_STEP = 2
EP = ("ep_0", "ep_1")
GRP_EP_TP = ("grp", "ep_0", "ep_1", "tp")
EP_TP = ("ep_0", "ep_1", "tp")
GRP_EP = ("grp", "ep_0", "ep_1")


rope_theta = 10000.0
norm_eps = 1e-06
routed_scale = 2.5
masked_score = -1e30


def device_at(row, col, core):
    return (row * 8 + col) * 2 + core


PLACES = [
    [
        device_at(2 * block_row + i, 2 * block_col + j, core)
        for block_row in range(4)
        for block_col in range(4)
    ]
    for i in range(2)
    for j in range(2)
    for core in range(2)
]


def partners(flip_i, flip_j):
    return [
        (device_at(row, col, core), device_at(row ^ flip_i, col ^ flip_j, core))
        for row in range(8)
        for col in range(8)
        for core in range(2)
    ]


def from_partner(array, flip):
    return lax.ppermute(array, EP_TP, partners(flip // 2, flip % 2))


def exchanged(blocks, groups):
    return lax.all_to_all(blocks, EP_TP, 0, 0, axis_index_groups=groups, tiled=True)


def sent_to_all(array, groups):
    count = len(groups[0])
    return exchanged(jnp.broadcast_to(array[None], (count, *array.shape)), groups)


def from_other_core(array):
    return lax.ppermute(array, "tp", [(0, 1), (1, 0)])


def normalize(values):
    return values * lax.rsqrt(jnp.mean(values * values, axis=-1, keepdims=True) + norm_eps)


def swiglu(flat_rows, gate_w, up_w, down_w):
    gate_part = jnp.dot(flat_rows, gate_w, preferred_element_type=jnp.float32)
    up_part = jnp.dot(flat_rows, up_w, preferred_element_type=jnp.float32)
    inner_rows = (jax.nn.silu(gate_part) * up_part).astype(jnp.bfloat16)
    return jnp.dot(inner_rows, down_w, preferred_element_type=jnp.float32).astype(jnp.bfloat16)


def attention_kernel(
    lengths_ref,
    nope_ref,
    rope_ref,
    latent_ref,
    key_ref,
    cosine_ref,
    sine_ref,
    absorb_ref,
    cache_ref,
    cache_rope_ref,
    out_ref,
    query_ref,
    query_pe_ref,
    latent_new_ref,
    key_new_ref,
):
    step = pl.program_id(0)
    seq_count, heads, nope = nope_ref.shape
    rope = rope_ref.shape[-1]
    half = rope // 2
    latent = cache_ref.shape[-1]
    scale = (nope + rope) ** (-0.5)

    def turned(values, cosine, sine):
        swapped = jnp.concatenate([values[..., half:], values[..., :half]], axis=-1)
        return values * cosine + swapped * sine

    @pl.when(step == 0)
    def _():
        rows = nope_ref[...].reshape(seq_count * heads, nope)
        twice = jnp.concatenate([rows, rows], axis=-1)
        wide = jnp.concatenate([twice] * (heads // 2), axis=-1)
        row_head = lax.broadcasted_iota(jnp.int32, wide.shape, 0) % heads
        column_head = lax.broadcasted_iota(jnp.int32, wide.shape, 1) // nope
        wide = jnp.where(row_head == column_head, wide.astype(jnp.float32), 0.0)
        queries = jnp.dot(
            wide.astype(jnp.bfloat16), absorb_ref[...], preferred_element_type=jnp.float32
        )
        query_ref[...] = queries.reshape(seq_count, heads, latent).astype(jnp.bfloat16)
        cosine = cosine_ref[...][:, None, :]
        sine = sine_ref[...][:, None, :]
        query_pe_ref[...] = turned(rope_ref[...].astype(jnp.float32), cosine, sine).astype(
            jnp.bfloat16
        )
        latent_new = normalize(latent_ref[...].astype(jnp.float32)).astype(jnp.bfloat16)
        latent_new_ref[...] = latent_new.astype(jnp.float32)[:, None, :]
        key_new = turned(key_ref[...].astype(jnp.float32), cosine_ref[...], sine_ref[...])
        key_new_ref[...] = key_new.astype(jnp.bfloat16).astype(jnp.float32)[:, None, :]

    for place in range(cache_ref.shape[0]):
        seq = step * cache_ref.shape[0] + place
        length = lengths_ref[seq]
        query = query_ref[seq]
        query_pe = query_pe_ref[seq]
        latent_wide = latent_new_ref[seq]
        score_new = (
            jnp.sum(query.astype(jnp.float32) * latent_wide, axis=-1, keepdims=True)
            + jnp.sum(query_pe.astype(jnp.float32) * key_new_ref[seq], axis=-1, keepdims=True)
        ) * scale
        cache = cache_ref[place]
        scores = (
            lax.dot_general(
                query, cache, (((1,), (1,)), ((), ())), preferred_element_type=jnp.float32
            )
            + jnp.dot(query_pe, cache_rope_ref[place], preferred_element_type=jnp.float32)
        ) * scale
        position = lax.broadcasted_iota(jnp.int32, scores.shape, 1)
        scores = jnp.where(position < length, scores, masked_score)
        row_max = jnp.maximum(jnp.max(scores, axis=-1, keepdims=True), score_new)
        weights = jnp.exp(scores - row_max)
        weight_new = jnp.exp(score_new - row_max)
        total = jnp.sum(weights, axis=-1, keepdims=True) + weight_new
        summed = (
            jnp.dot(weights.astype(jnp.bfloat16), cache, preferred_element_type=jnp.float32)
            + weight_new.astype(jnp.bfloat16).astype(jnp.float32) * latent_wide
        )
        out_ref[place] = (summed / total).astype(jnp.bfloat16)


def attended(query_nope, query_rope, new_latent, new_rope, cache_latent, cache_rope, lengths, absorb_key):
    seq_count, heads, nope = query_nope.shape
    rope = query_rope.shape[-1]
    latent = cache_latent.shape[-1]
    context = cache_latent.shape[1]
    half = rope // 2
    inverse = rope_theta ** (-jnp.arange(half, dtype=jnp.float32) * 2.0 / rope)
    angles = lengths.astype(jnp.float32)[:, None] * jnp.concatenate([inverse, inverse])[None, :]
    sign = jnp.where(jnp.arange(rope) < half, -1.0, 1.0)
    cosine = jnp.cos(angles)
    sine = jnp.sin(angles) * sign[None, :]
    absorb = absorb_key.transpose(1, 2, 0).reshape(heads * nope, latent)
    rope_turned = cache_rope.transpose(0, 2, 1)
    whole = lambda *shape: pl.BlockSpec(shape, lambda step, lengths: (0,) * len(shape))
    return pl.pallas_call(
        attention_kernel,
        grid_spec=pltpu.PrefetchScalarGridSpec(
            num_scalar_prefetch=1,
            grid=(seq_count // SEQ_STEP,),
            in_specs=[
                whole(seq_count, heads, nope),
                whole(seq_count, heads, rope),
                whole(seq_count, latent),
                whole(seq_count, rope),
                whole(seq_count, rope),
                whole(seq_count, rope),
                whole(heads * nope, latent),
                pl.BlockSpec((SEQ_STEP, context, latent), lambda step, lengths: (step, 0, 0)),
                pl.BlockSpec((SEQ_STEP, rope, context), lambda step, lengths: (step, 0, 0)),
            ],
            out_specs=pl.BlockSpec((SEQ_STEP, heads, latent), lambda step, lengths: (step, 0, 0)),
            scratch_shapes=[
                pltpu.VMEM((seq_count, heads, latent), jnp.bfloat16),
                pltpu.VMEM((seq_count, heads, rope), jnp.bfloat16),
                pltpu.VMEM((seq_count, 1, latent), jnp.float32),
                pltpu.VMEM((seq_count, 1, rope), jnp.float32),
            ],
        ),
        out_shape=jax.ShapeDtypeStruct((seq_count, heads, latent), jnp.bfloat16),
        compiler_params=pltpu.CompilerParams(dimension_semantics=("arbitrary",)),
        cost_estimate=pl.CostEstimate(
            flops=8 * seq_count * heads * context * latent,
            bytes_accessed=2 * seq_count * context * (latent + rope),
            transcendentals=seq_count * heads * context,
        ),
        name="attended",
    )(
        lengths, query_nope, query_rope, new_latent, new_rope, cosine, sine, absorb, cache_latent, rope_turned
    )


def attention(
    query_nope,
    query_rope,
    new_latent,
    new_rope,
    cache_latent,
    cache_rope,
    lengths,
    absorb_key,
    value_up,
):
    latent_out = attended(
        query_nope, query_rope, new_latent, new_rope, cache_latent, cache_rope, lengths, absorb_key
    )
    return (
        jnp.einsum("shc,chv->shv", latent_out, value_up, preferred_element_type=jnp.float32)
        .astype(jnp.bfloat16)
        .reshape(latent_out.shape[0], -1)
    )


def spread_kernel(
    place_ref,
    pieces_ref,
    hidden_ref,
    gain_mix_ref,
    gain_in_ref,
    routes_ref,
    outgoing_ref,
    ffn_ref,
    mix_ref,
    taken_ref,
):
    core, block_i, block_j = place_ref[0], place_ref[1], place_ref[2]
    rows, _ = hidden_ref.shape
    piece = pieces_ref.shape[-1]
    run = piece // 4
    chunks = []
    for block_row in range(4):
        for i in range(2):
            runs = [
                pieces_ref[
                    c,
                    (i ^ block_i) * 2 + (j ^ block_j),
                    :,
                    block_row * run : (block_row + 1) * run,
                ]
                for j in range(2)
                for c in range(2)
            ]
            chunks.append(jnp.concatenate(runs, axis=-1))
    joined = jnp.concatenate(chunks, axis=0)
    source = lax.broadcasted_iota(jnp.int32, (piece, piece), 0)
    target = lax.broadcasted_iota(jnp.int32, (piece, piece), 1)
    k = run // 4
    goes_to = (source % run) // k * run + source // run * k + source % k
    order = jnp.where(goes_to == target, 1.0, 0.0).astype(jnp.bfloat16)
    placed = jnp.dot(joined, order, preferred_element_type=jnp.float32)
    mixed = jnp.concatenate(
        [placed[n * rows : (n + 1) * rows] for n in range(len(chunks))], axis=-1
    )
    after_mix = (
        hidden_ref[...].astype(jnp.float32)
        + gain_mix_ref[...].astype(jnp.float32) * normalize(mixed)
    ).astype(jnp.bfloat16)
    after_wide = after_mix.astype(jnp.float32)
    ffn_in = (normalize(after_wide) * gain_in_ref[...].astype(jnp.float32)).astype(jnp.bfloat16)
    ffn_ref[...] = ffn_in
    half = rows // 2
    mix_ref[...] = jnp.where(core == 0, after_wide[:half], after_wide[half:]).astype(jnp.bfloat16)
    slots = outgoing_ref.shape[0]
    slot = lax.broadcasted_iota(jnp.int32, (rows, slots), 1)
    expert = slot // 2 * 2 + core
    named = jnp.zeros((rows, slots), jnp.float32)
    for n in range(routes_ref.shape[1]):
        named = jnp.where(routes_ref[:, n : n + 1] == expert, 1.0, named)
    earlier = jnp.where(
        lax.broadcasted_iota(jnp.int32, (rows, rows), 1)
        < lax.broadcasted_iota(jnp.int32, (rows, rows), 0),
        1.0,
        0.0,
    ).astype(jnp.bfloat16)
    before = jnp.dot(earlier, named.astype(jnp.bfloat16), preferred_element_type=jnp.float32)
    taken = jnp.where(before == (slot % 2).astype(jnp.float32), named, 0.0).astype(jnp.bfloat16)
    taken_ref[...] = taken
    outgoing_ref[...] = lax.dot_general(
        taken, ffn_in, (((0,), (0,)), ((), ())), preferred_element_type=jnp.float32
    ).astype(jnp.bfloat16)


def spread(place, pieces, chip_hidden, gain_mix, gain_in, routes, slots):
    rows, width = chip_hidden.shape
    return pl.pallas_call(
        spread_kernel,
        in_specs=[pl.BlockSpec(memory_space=pltpu.SMEM)]
        + [pl.BlockSpec(memory_space=pltpu.VMEM)] * 5,
        out_specs=[pl.BlockSpec(memory_space=pltpu.VMEM)] * 4,
        out_shape=[
            jax.ShapeDtypeStruct((slots, width), jnp.bfloat16),
            jax.ShapeDtypeStruct((rows, width), jnp.bfloat16),
            jax.ShapeDtypeStruct((rows // 2, width), jnp.bfloat16),
            jax.ShapeDtypeStruct((rows, slots), jnp.bfloat16),
        ],
        name="spread",
    )(place, pieces, chip_hidden, gain_mix[None], gain_in[None], routes)


def local(
    hidden_in,
    query_nope,
    query_rope,
    new_latent,
    new_rope,
    cache_latent,
    cache_rope,
    lengths,
    absorb_key,
    value_up,
    out_proj,
    gain_mix,
    gain_ffn_in,
    router,
    routes,
    expert_gate,
    expert_up,
    expert_down,
    shared_gate,
    shared_up,
    shared_down,
    gain_ffn_out,
):
    seq_count, width = hidden_in.shape
    core = lax.axis_index("tp")
    own_start = core * seq_count
    slab = sent_to_all(out_proj.T, PLACES).reshape(-1, out_proj.shape[0])
    chip_hidden = lax.all_gather(hidden_in, "tp", axis=0, tiled=True)
    heads_out = attention(
        query_nope,
        query_rope,
        new_latent,
        new_rope,
        cache_latent,
        cache_rope,
        lengths,
        absorb_key,
        value_up,
    )
    chip_heads = lax.all_gather(heads_out, "tp", axis=0, tiled=True)
    block_heads = jnp.concatenate(
        [chip_heads] + [from_partner(chip_heads, flip) for flip in range(1, 4)], axis=0
    )
    partial = lax.dot_general(
        block_heads, slab, (((1,), (1,)), ((), ())), preferred_element_type=jnp.float32
    ).astype(jnp.bfloat16)
    chip_rows = partial.reshape(4, 2 * seq_count, -1)
    pieces = jnp.stack(
        [chip_rows[0]] + [from_partner(chip_rows[flip], flip) for flip in range(1, 4)]
    )
    pieces = lax.all_gather(pieces, "tp", axis=0)
    place = jnp.stack([core, lax.axis_index("ep_0") % 2, lax.axis_index("ep_1") % 2])
    experts_total = router.shape[1]
    group_rows, top_count = routes.shape
    ep_count = lax.axis_size(EP)
    capacity = 2 * ((group_rows * top_count + experts_total - 1) // experts_total)
    slots = ep_count * capacity
    slot_expert = lax.iota(jnp.int32, slots) // capacity * 2 + core
    outgoing, ffn_in, own_mix, taken = spread(
        place.astype(jnp.int32), pieces, chip_hidden, gain_mix, gain_ffn_in, routes, slots
    )
    received = lax.all_to_all(
        outgoing.reshape(ep_count, capacity, width), EP, split_axis=0, concat_axis=0, tiled=True
    )
    affinity = jax.nn.sigmoid(jnp.dot(ffn_in, router, preferred_element_type=jnp.float32))
    choose = routes[..., None] == lax.iota(jnp.int32, experts_total)[None, None, :]
    chosen = jnp.sum(jnp.where(choose, affinity[:, None, :], 0.0), axis=-1)
    route_weights = chosen / jnp.sum(chosen, axis=-1, keepdims=True) * routed_scale
    slot_weights = jnp.sum(
        jnp.where(
            routes[:, :, None] == slot_expert[None, None, :], route_weights[:, :, None], 0.0
        ),
        axis=1,
    )
    slot_weights = slot_weights * taken.astype(jnp.float32)
    weights_high = slot_weights.astype(jnp.bfloat16)
    weights_low = (slot_weights - weights_high.astype(jnp.float32)).astype(jnp.bfloat16)
    own_ffn = lax.dynamic_slice_in_dim(ffn_in, own_start, seq_count, 0)
    shared = swiglu(own_ffn, shared_gate, shared_up, shared_down)
    outputs = swiglu(
        received.reshape(slots, width), expert_gate[0], expert_up[0], expert_down[0]
    )
    returned = lax.all_to_all(
        outputs.reshape(ep_count, capacity, width), EP, split_axis=0, concat_axis=0, tiled=True
    ).reshape(slots, width)
    both = jnp.dot(
        jnp.concatenate([weights_high, weights_low], axis=0),
        returned,
        preferred_element_type=jnp.float32,
    )
    routed = both[:group_rows] + both[group_rows:]
    kept = lax.dynamic_slice_in_dim(routed, own_start, seq_count, 0)
    given = lax.dynamic_slice_in_dim(routed, seq_count - own_start, seq_count, 0)
    combined = kept + from_other_core(given) + shared.astype(jnp.float32)
    return (
        own_mix.astype(jnp.float32) + gain_ffn_out.astype(jnp.float32) * normalize(combined)
    ).astype(jnp.bfloat16)


def solution(mesh):
    torus = Mesh(
        mesh.devices.reshape(mesh.shape["grp"], 8, 8, mesh.shape["tp"]),
        ("grp", "ep_0", "ep_1", "tp"),
    )
    in_specs = (
        P(GRP_EP_TP, None),
        P(GRP_EP_TP, None, None),
        P(GRP_EP_TP, None, None),
        P(GRP_EP_TP, None),
        P(GRP_EP_TP, None),
        P(GRP_EP_TP, None, None),
        P(GRP_EP_TP, None, None),
        P(GRP_EP_TP),
        P(),
        P(),
        P(None, EP_TP),
        P(),
        P(),
        P(),
        P(GRP_EP, None),
        P(EP_TP, None, None),
        P(EP_TP, None, None),
        P(EP_TP, None, None),
        P(),
        P(),
        P(),
        P(),
    )
    out_specs = P(GRP_EP_TP, None)

    return jax.shard_map(local, mesh=torus, in_specs=in_specs, out_specs=out_specs, check_vma=False)
```

```python
import jax
import jax.numpy as jnp
from jax import lax
from jax.experimental import pallas as pl
from jax.experimental.pallas import tpu as pltpu
from jax.sharding import Mesh
from jax.sharding import PartitionSpec as P

SEQ_STEP = 2
EP = ("ep_0", "ep_1")
GRP_EP_TP = ("grp", "ep_0", "ep_1", "tp")
EP_TP = ("ep_0", "ep_1", "tp")
GRP_EP = ("grp", "ep_0", "ep_1")


rope_theta = 10000.0
norm_eps = 1e-06
routed_scale = 2.5
masked_score = -1e30


def device_at(row, col, core):
    return (row * 8 + col) * 2 + core


PLACES = [
    [
        device_at(2 * block_row + i, 2 * block_col + j, core)
        for block_row in range(4)
        for block_col in range(4)
    ]
    for i in range(2)
    for j in range(2)
    for core in range(2)
]


def partners(flip_i, flip_j):
    return [
        (device_at(row, col, core), device_at(row ^ flip_i, col ^ flip_j, core))
        for row in range(8)
        for col in range(8)
        for core in range(2)
    ]


def from_partner(array, flip):
    return lax.ppermute(array, EP_TP, partners(flip // 2, flip % 2))


def exchanged(blocks, groups):
    return lax.all_to_all(blocks, EP_TP, 0, 0, axis_index_groups=groups, tiled=True)


def sent_to_all(array, groups):
    count = len(groups[0])
    return exchanged(jnp.broadcast_to(array[None], (count, *array.shape)), groups)


def from_other_core(array):
    return lax.ppermute(array, "tp", [(0, 1), (1, 0)])


def normalize(values):
    return values * lax.rsqrt(jnp.mean(values * values, axis=-1, keepdims=True) + norm_eps)


def swiglu(flat_rows, gate_w, up_w, down_w):
    gate_part = jnp.dot(flat_rows, gate_w, preferred_element_type=jnp.float32)
    up_part = jnp.dot(flat_rows, up_w, preferred_element_type=jnp.float32)
    inner_rows = (jax.nn.silu(gate_part) * up_part).astype(jnp.bfloat16)
    return jnp.dot(inner_rows, down_w, preferred_element_type=jnp.float32).astype(jnp.bfloat16)


def attention_kernel(
    lengths_ref,
    nope_ref,
    rope_ref,
    latent_ref,
    key_ref,
    cosine_ref,
    sine_ref,
    absorb_ref,
    cache_ref,
    cache_rope_ref,
    out_ref,
    query_ref,
    query_pe_ref,
    latent_new_ref,
    key_new_ref,
):
    step = pl.program_id(0)
    seq_count, heads, nope = nope_ref.shape
    rope = rope_ref.shape[-1]
    half = rope // 2
    latent = cache_ref.shape[-1]
    scale = (nope + rope) ** (-0.5)

    def turned(values, cosine, sine):
        swapped = jnp.concatenate([values[..., half:], values[..., :half]], axis=-1)
        return values * cosine + swapped * sine

    @pl.when(step == 0)
    def _():
        rows = nope_ref[...].reshape(seq_count * heads, nope)
        twice = jnp.concatenate([rows, rows], axis=-1)
        wide = jnp.concatenate([twice] * (heads // 2), axis=-1)
        row_head = lax.broadcasted_iota(jnp.int32, wide.shape, 0) % heads
        column_head = lax.broadcasted_iota(jnp.int32, wide.shape, 1) // nope
        wide = jnp.where(row_head == column_head, wide.astype(jnp.float32), 0.0)
        queries = jnp.dot(
            wide.astype(jnp.bfloat16), absorb_ref[...], preferred_element_type=jnp.float32
        )
        query_ref[...] = queries.reshape(seq_count, heads, latent).astype(jnp.bfloat16)
        cosine = cosine_ref[...][:, None, :]
        sine = sine_ref[...][:, None, :]
        query_pe_ref[...] = turned(rope_ref[...].astype(jnp.float32), cosine, sine).astype(
            jnp.bfloat16
        )
        latent_new = normalize(latent_ref[...].astype(jnp.float32)).astype(jnp.bfloat16)
        latent_new_ref[...] = latent_new.astype(jnp.float32)[:, None, :]
        key_new = turned(key_ref[...].astype(jnp.float32), cosine_ref[...], sine_ref[...])
        key_new_ref[...] = key_new.astype(jnp.bfloat16).astype(jnp.float32)[:, None, :]

    for place in range(cache_ref.shape[0]):
        seq = step * cache_ref.shape[0] + place
        length = lengths_ref[seq]
        query = query_ref[seq]
        query_pe = query_pe_ref[seq]
        latent_wide = latent_new_ref[seq]
        score_new = (
            jnp.sum(query.astype(jnp.float32) * latent_wide, axis=-1, keepdims=True)
            + jnp.sum(query_pe.astype(jnp.float32) * key_new_ref[seq], axis=-1, keepdims=True)
        ) * scale
        cache = cache_ref[place]
        scores = (
            lax.dot_general(
                query, cache, (((1,), (1,)), ((), ())), preferred_element_type=jnp.float32
            )
            + jnp.dot(query_pe, cache_rope_ref[place], preferred_element_type=jnp.float32)
        ) * scale
        position = lax.broadcasted_iota(jnp.int32, scores.shape, 1)
        scores = jnp.where(position < length, scores, masked_score)
        row_max = jnp.maximum(jnp.max(scores, axis=-1, keepdims=True), score_new)
        weights = jnp.exp(scores - row_max)
        weight_new = jnp.exp(score_new - row_max)
        total = jnp.sum(weights, axis=-1, keepdims=True) + weight_new
        summed = (
            jnp.dot(weights.astype(jnp.bfloat16), cache, preferred_element_type=jnp.float32)
            + weight_new.astype(jnp.bfloat16).astype(jnp.float32) * latent_wide
        )
        out_ref[place] = (summed / total).astype(jnp.bfloat16)


def attended(query_nope, query_rope, new_latent, new_rope, cache_latent, cache_rope, lengths, absorb_key):
    seq_count, heads, nope = query_nope.shape
    rope = query_rope.shape[-1]
    latent = cache_latent.shape[-1]
    context = cache_latent.shape[1]
    half = rope // 2
    inverse = rope_theta ** (-jnp.arange(half, dtype=jnp.float32) * 2.0 / rope)
    angles = lengths.astype(jnp.float32)[:, None] * jnp.concatenate([inverse, inverse])[None, :]
    sign = jnp.where(jnp.arange(rope) < half, -1.0, 1.0)
    cosine = jnp.cos(angles)
    sine = jnp.sin(angles) * sign[None, :]
    absorb = absorb_key.transpose(1, 2, 0).reshape(heads * nope, latent)
    rope_turned = cache_rope.transpose(0, 2, 1)
    whole = lambda *shape: pl.BlockSpec(shape, lambda step, lengths: (0,) * len(shape))
    return pl.pallas_call(
        attention_kernel,
        grid_spec=pltpu.PrefetchScalarGridSpec(
            num_scalar_prefetch=1,
            grid=(seq_count // SEQ_STEP,),
            in_specs=[
                whole(seq_count, heads, nope),
                whole(seq_count, heads, rope),
                whole(seq_count, latent),
                whole(seq_count, rope),
                whole(seq_count, rope),
                whole(seq_count, rope),
                whole(heads * nope, latent),
                pl.BlockSpec((SEQ_STEP, context, latent), lambda step, lengths: (step, 0, 0)),
                pl.BlockSpec((SEQ_STEP, rope, context), lambda step, lengths: (step, 0, 0)),
            ],
            out_specs=pl.BlockSpec((SEQ_STEP, heads, latent), lambda step, lengths: (step, 0, 0)),
            scratch_shapes=[
                pltpu.VMEM((seq_count, heads, latent), jnp.bfloat16),
                pltpu.VMEM((seq_count, heads, rope), jnp.bfloat16),
                pltpu.VMEM((seq_count, 1, latent), jnp.float32),
                pltpu.VMEM((seq_count, 1, rope), jnp.float32),
            ],
        ),
        out_shape=jax.ShapeDtypeStruct((seq_count, heads, latent), jnp.bfloat16),
        compiler_params=pltpu.CompilerParams(dimension_semantics=("arbitrary",), vmem_limit_bytes=60 * 1024 * 1024),
        cost_estimate=pl.CostEstimate(
            flops=8 * seq_count * heads * context * latent,
            bytes_accessed=2 * seq_count * context * (latent + rope),
            transcendentals=seq_count * heads * context,
        ),
        name="attended",
    )(
        lengths, query_nope, query_rope, new_latent, new_rope, cosine, sine, absorb, cache_latent, rope_turned
    )


def attention(
    query_nope,
    query_rope,
    new_latent,
    new_rope,
    cache_latent,
    cache_rope,
    lengths,
    absorb_key,
    value_up,
):
    latent_out = attended(
        query_nope, query_rope, new_latent, new_rope, cache_latent, cache_rope, lengths, absorb_key
    )
    return (
        jnp.einsum("shc,chv->shv", latent_out, value_up, preferred_element_type=jnp.float32)
        .astype(jnp.bfloat16)
        .reshape(latent_out.shape[0], -1)
    )


def spread_kernel(
    place_ref,
    pieces_ref,
    hidden_ref,
    gain_mix_ref,
    gain_in_ref,
    routes_ref,
    outgoing_ref,
    ffn_ref,
    mix_ref,
    taken_ref,
):
    core, block_i, block_j = place_ref[0], place_ref[1], place_ref[2]
    rows, _ = hidden_ref.shape
    piece = pieces_ref.shape[-1]
    run = piece // 4
    chunks = []
    for block_row in range(4):
        for i in range(2):
            runs = [
                pieces_ref[
                    c,
                    (i ^ block_i) * 2 + (j ^ block_j),
                    :,
                    block_row * run : (block_row + 1) * run,
                ]
                for j in range(2)
                for c in range(2)
            ]
            chunks.append(jnp.concatenate(runs, axis=-1))
    joined = jnp.concatenate(chunks, axis=0)
    source = lax.broadcasted_iota(jnp.int32, (piece, piece), 0)
    target = lax.broadcasted_iota(jnp.int32, (piece, piece), 1)
    k = run // 4
    goes_to = (source % run) // k * run + source // run * k + source % k
    order = jnp.where(goes_to == target, 1.0, 0.0).astype(jnp.bfloat16)
    placed = jnp.dot(joined, order, preferred_element_type=jnp.float32)
    mixed = jnp.concatenate(
        [placed[n * rows : (n + 1) * rows] for n in range(len(chunks))], axis=-1
    )
    after_mix = (
        hidden_ref[...].astype(jnp.float32)
        + gain_mix_ref[...].astype(jnp.float32)[None] * normalize(mixed)
    ).astype(jnp.bfloat16)
    after_wide = after_mix.astype(jnp.float32)
    ffn_in = (normalize(after_wide) * gain_in_ref[...].astype(jnp.float32)[None]).astype(jnp.bfloat16)
    ffn_ref[...] = ffn_in
    half = rows // 2
    mix_ref[...] = jnp.where(core == 0, after_wide[:half], after_wide[half:]).astype(jnp.bfloat16)
    slots = taken_ref.shape[0]
    slot = lax.broadcasted_iota(jnp.int32, (slots, rows), 0)
    expert = slot // 2 * 2 + core
    named = jnp.zeros((slots, rows), jnp.float32)
    for n in range(routes_ref.shape[0]):
        named = jnp.where(routes_ref[n : n + 1, :] == expert, 1.0, named)
    earlier = jnp.where(
        lax.broadcasted_iota(jnp.int32, (rows, rows), 0)
        < lax.broadcasted_iota(jnp.int32, (rows, rows), 1),
        1.0,
        0.0,
    ).astype(jnp.bfloat16)
    before = jnp.dot(named.astype(jnp.bfloat16), earlier, preferred_element_type=jnp.float32)
    taken = jnp.where(before == (slot % 2).astype(jnp.float32), named, 0.0).astype(jnp.bfloat16)
    taken_ref[...] = taken
    outgoing = jnp.dot(taken, ffn_in, preferred_element_type=jnp.float32).astype(jnp.bfloat16)
    outgoing_ref[...] = outgoing.reshape(outgoing_ref.shape)


def spread(place, pieces, chip_hidden, gain_mix, gain_in, routes, slots):
    rows, width = chip_hidden.shape
    return pl.pallas_call(
        spread_kernel,
        in_specs=[pl.BlockSpec(memory_space=pltpu.SMEM)]
        + [pl.BlockSpec(memory_space=pltpu.VMEM)] * 5,
        out_specs=[pl.BlockSpec(memory_space=pltpu.VMEM)] * 4,
        out_shape=[
            jax.ShapeDtypeStruct((slots // 2, 2, width), jnp.bfloat16),
            jax.ShapeDtypeStruct((rows, width), jnp.bfloat16),
            jax.ShapeDtypeStruct((rows // 2, width), jnp.bfloat16),
            jax.ShapeDtypeStruct((slots, rows), jnp.bfloat16),
        ],
        compiler_params=pltpu.CompilerParams(vmem_limit_bytes=8 << 20),
        name="spread",
    )(place, pieces, chip_hidden, gain_mix, gain_in, routes.T)


def experts_kernel(rows_ref, gate_ref, up_ref, down_ref, out_ref):
    rows = rows_ref[...]
    gate_part = jnp.dot(rows, gate_ref[...], preferred_element_type=jnp.float32)
    up_part = jnp.dot(rows, up_ref[...], preferred_element_type=jnp.float32)
    inner = (gate_part / (1.0 + jnp.exp(-gate_part)) * up_part).astype(jnp.bfloat16)
    out_ref[...] = jnp.dot(inner, down_ref[...], preferred_element_type=jnp.float32).astype(
        out_ref.dtype
    )


def expert_rows(rows, gate_w, up_w, down_w):
    return pl.pallas_call(
        experts_kernel,
        in_specs=[pl.BlockSpec(memory_space=pltpu.VMEM)] * 4,
        out_specs=pl.BlockSpec(memory_space=pltpu.VMEM),
        out_shape=jax.ShapeDtypeStruct((rows.shape[0], down_w.shape[1]), jnp.bfloat16),
        compiler_params=pltpu.CompilerParams(vmem_limit_bytes=10 << 20),
    )(rows, gate_w, up_w, down_w)


def local(
    hidden_in,
    query_nope,
    query_rope,
    new_latent,
    new_rope,
    cache_latent,
    cache_rope,
    lengths,
    absorb_key,
    value_up,
    out_proj,
    gain_mix,
    gain_ffn_in,
    router,
    routes,
    expert_gate,
    expert_up,
    expert_down,
    shared_gate,
    shared_up,
    shared_down,
    gain_ffn_out,
):
    seq_count, width = hidden_in.shape
    core = lax.axis_index("tp")
    own_start = core * seq_count
    slab = sent_to_all(out_proj.T, PLACES).reshape(-1, out_proj.shape[0])
    chip_hidden = lax.all_gather(hidden_in, "tp", axis=0, tiled=True)
    heads_out = attention(
        query_nope,
        query_rope,
        new_latent,
        new_rope,
        cache_latent,
        cache_rope,
        lengths,
        absorb_key,
        value_up,
    )
    chip_heads = lax.all_gather(heads_out, "tp", axis=0, tiled=True)
    block_heads = jnp.concatenate(
        [chip_heads] + [from_partner(chip_heads, flip) for flip in range(1, 4)], axis=0
    )
    partial = lax.dot_general(
        block_heads, slab, (((1,), (1,)), ((), ())), preferred_element_type=jnp.float32
    ).astype(jnp.bfloat16)
    chip_rows = partial.reshape(4, 2 * seq_count, -1)
    pieces = jnp.stack(
        [chip_rows[0]] + [from_partner(chip_rows[flip], flip) for flip in range(1, 4)]
    )
    pieces = lax.all_gather(pieces, "tp", axis=0)
    place = jnp.stack([core, lax.axis_index("ep_0") % 2, lax.axis_index("ep_1") % 2])
    experts_total = router.shape[1]
    group_rows, top_count = routes.shape
    ep_count = lax.axis_size(EP)
    capacity = 2 * ((group_rows * top_count + experts_total - 1) // experts_total)
    slots = ep_count * capacity
    slot_expert = lax.iota(jnp.int32, slots) // capacity * 2 + core
    outgoing, ffn_in, own_mix, taken = spread(
        place.astype(jnp.int32), pieces, chip_hidden, gain_mix, gain_ffn_in, routes, slots
    )
    received = lax.all_to_all(
        outgoing, EP, split_axis=0, concat_axis=0, tiled=True
    )
    affinity = jax.nn.sigmoid(jnp.dot(ffn_in, router, preferred_element_type=jnp.float32))
    choose = routes[..., None] == lax.iota(jnp.int32, experts_total)[None, None, :]
    chosen = jnp.sum(jnp.where(choose, affinity[:, None, :], 0.0), axis=-1)
    route_weights = chosen / jnp.sum(chosen, axis=-1, keepdims=True) * routed_scale
    slot_weights = jnp.sum(
        jnp.where(
            routes[:, :, None] == slot_expert[None, None, :], route_weights[:, :, None], 0.0
        ),
        axis=1,
    )
    slot_weights = slot_weights * taken.T.astype(jnp.float32)
    weights_high = slot_weights.astype(jnp.bfloat16)
    weights_low = (slot_weights - weights_high.astype(jnp.float32)).astype(jnp.bfloat16)
    own_ffn = lax.dynamic_slice_in_dim(ffn_in, own_start, seq_count, 0)
    shared = expert_rows(own_ffn, shared_gate, shared_up, shared_down)
    outputs = swiglu(
        received.reshape(slots, width), expert_gate[0], expert_up[0], expert_down[0]
    )
    returned = lax.all_to_all(
        outputs.reshape(ep_count, capacity, width), EP, split_axis=0, concat_axis=0, tiled=True
    ).reshape(slots, width)
    both = jnp.dot(
        jnp.concatenate([weights_high, weights_low], axis=0),
        returned,
        preferred_element_type=jnp.float32,
    )
    routed = both[:group_rows] + both[group_rows:]
    kept = lax.dynamic_slice_in_dim(routed, own_start, seq_count, 0)
    given = lax.dynamic_slice_in_dim(routed, seq_count - own_start, seq_count, 0)
    combined = kept + from_other_core(given) + shared.astype(jnp.float32)
    return (
        own_mix.astype(jnp.float32) + gain_ffn_out.astype(jnp.float32) * normalize(combined)
    ).astype(jnp.bfloat16)


def solution(mesh):
    torus = Mesh(
        mesh.devices.reshape(mesh.shape["grp"], 8, 8, mesh.shape["tp"]),
        ("grp", "ep_0", "ep_1", "tp"),
    )
    in_specs = (
        P(GRP_EP_TP, None),
        P(GRP_EP_TP, None, None),
        P(GRP_EP_TP, None, None),
        P(GRP_EP_TP, None),
        P(GRP_EP_TP, None),
        P(GRP_EP_TP, None, None),
        P(GRP_EP_TP, None, None),
        P(GRP_EP_TP),
        P(),
        P(),
        P(None, EP_TP),
        P(),
        P(),
        P(),
        P(GRP_EP, None),
        P(EP_TP, None, None),
        P(EP_TP, None, None),
        P(EP_TP, None, None),
        P(),
        P(),
        P(),
        P(),
    )
    out_specs = P(GRP_EP_TP, None)

    return jax.shard_map(local, mesh=torus, in_specs=in_specs, out_specs=out_specs, check_vma=False)
```

```python
import math

import jax
import jax.numpy as jnp
from jax import lax
from jax.experimental import pallas as pl
from jax.experimental.pallas import tpu as pltpu
from jax.sharding import Mesh
from jax.sharding import PartitionSpec as P

SEQ_STEP = 2
EP = ("ep_0", "ep_1")
GRP_EP_TP = ("grp", "ep_0", "ep_1", "tp")
EP_TP = ("ep_0", "ep_1", "tp")
GRP_EP = ("grp", "ep_0", "ep_1")


rope_theta = 10000.0
norm_eps = 1e-06
routed_scale = 2.5
masked_score = -1e30


def device_at(row, col, core):
    return (row * 8 + col) * 2 + core


PLACES = [
    [
        device_at(2 * block_row + i, 2 * block_col + j, core)
        for block_row in range(4)
        for block_col in range(4)
    ]
    for i in range(2)
    for j in range(2)
    for core in range(2)
]


def partners(flip_i, flip_j):
    return [
        (device_at(row, col, core), device_at(row ^ flip_i, col ^ flip_j, core))
        for row in range(8)
        for col in range(8)
        for core in range(2)
    ]


def from_partner(array, flip):
    return lax.ppermute(array, EP_TP, partners(flip // 2, flip % 2))


def exchanged(blocks, groups):
    return lax.all_to_all(blocks, EP_TP, 0, 0, axis_index_groups=groups, tiled=True)


def sent_to_all(array, groups):
    count = len(groups[0])
    return exchanged(jnp.broadcast_to(array[None], (count, *array.shape)), groups)


def from_other_core(array):
    return lax.ppermute(array, "tp", [(0, 1), (1, 0)])


def normalize(values):
    return values * lax.rsqrt(jnp.mean(values * values, axis=-1, keepdims=True) + norm_eps)


def attention_kernel(
    lengths_ref,
    nope_ref,
    rope_ref,
    latent_ref,
    key_ref,
    absorb_ref,
    cache_ref,
    cache_rope_ref,
    out_ref,
    query_ref,
    query_pe_ref,
    latent_new_ref,
    key_new_ref,
):
    step = pl.program_id(0)
    seq_count, heads, nope = nope_ref.shape
    rope = rope_ref.shape[-1]
    half = rope // 2
    latent = cache_ref.shape[-1]
    scale = (nope + rope) ** (-0.5)

    def turned(values, cosine, sine):
        swapped = jnp.concatenate([values[..., half:], values[..., :half]], axis=-1)
        return values * cosine + swapped * sine

    @pl.when(step == 0)
    def _():
        rows = nope_ref[...].reshape(seq_count * heads, nope)
        twice = jnp.concatenate([rows, rows], axis=-1)
        wide = jnp.concatenate([twice] * (heads // 2), axis=-1)
        row_head = lax.broadcasted_iota(jnp.int32, wide.shape, 0) % heads
        column_head = lax.broadcasted_iota(jnp.int32, wide.shape, 1) // nope
        wide = jnp.where(row_head == column_head, wide.astype(jnp.float32), 0.0)
        queries = jnp.dot(
            wide.astype(jnp.bfloat16), absorb_ref[...], preferred_element_type=jnp.float32
        )
        query_ref[...] = queries.reshape(seq_count, heads, latent).astype(jnp.bfloat16)
        row = lax.broadcasted_iota(jnp.int32, (seq_count, rope), 0)
        column = lax.broadcasted_iota(jnp.int32, (seq_count, rope), 1)
        position = jnp.zeros((seq_count, rope), jnp.int32)
        for n in range(seq_count):
            position = jnp.where(row == n, lengths_ref[n], position)
        exponent = (column % half).astype(jnp.float32) * (-2.0 / rope * math.log(rope_theta))
        angles = position.astype(jnp.float32) * jnp.exp(exponent)
        cosine = jnp.cos(angles)
        sine = jnp.sin(angles)
        sine = jnp.where(column < half, -sine, sine)
        query_pe_ref[...] = turned(
            rope_ref[...].astype(jnp.float32), cosine[:, None, :], sine[:, None, :]
        ).astype(jnp.bfloat16)
        latent_new = normalize(latent_ref[...].astype(jnp.float32)).astype(jnp.bfloat16)
        latent_new_ref[...] = latent_new.astype(jnp.float32)[:, None, :]
        key_new = turned(key_ref[...].astype(jnp.float32), cosine, sine)
        key_new_ref[...] = key_new.astype(jnp.bfloat16).astype(jnp.float32)[:, None, :]

    for place in range(cache_ref.shape[0]):
        seq = step * cache_ref.shape[0] + place
        length = lengths_ref[seq]
        query = query_ref[seq]
        query_pe = query_pe_ref[seq]
        latent_wide = latent_new_ref[seq]
        score_new = (
            jnp.sum(query.astype(jnp.float32) * latent_wide, axis=-1, keepdims=True)
            + jnp.sum(query_pe.astype(jnp.float32) * key_new_ref[seq], axis=-1, keepdims=True)
        ) * scale
        cache = cache_ref[place]
        scores = (
            lax.dot_general(
                query, cache, (((1,), (1,)), ((), ())), preferred_element_type=jnp.float32
            )
            + jnp.dot(query_pe, cache_rope_ref[place], preferred_element_type=jnp.float32)
        ) * scale
        position = lax.broadcasted_iota(jnp.int32, scores.shape, 1)
        scores = jnp.where(position < length, scores, masked_score)
        row_max = jnp.maximum(jnp.max(scores, axis=-1, keepdims=True), score_new)
        weights = jnp.exp(scores - row_max)
        weight_new = jnp.exp(score_new - row_max)
        total = jnp.sum(weights, axis=-1, keepdims=True) + weight_new
        summed = (
            jnp.dot(weights.astype(jnp.bfloat16), cache, preferred_element_type=jnp.float32)
            + weight_new.astype(jnp.bfloat16).astype(jnp.float32) * latent_wide
        )
        out_ref[place] = (summed / total).astype(jnp.bfloat16)


def attended(query_nope, query_rope, new_latent, new_rope, cache_latent, cache_rope, lengths, absorb_key):
    seq_count, heads, nope = query_nope.shape
    rope = query_rope.shape[-1]
    latent = cache_latent.shape[-1]
    context = cache_latent.shape[1]
    absorb = absorb_key.transpose(1, 2, 0).reshape(heads * nope, latent)
    rope_turned = cache_rope.transpose(0, 2, 1)
    whole = lambda *shape: pl.BlockSpec(shape, lambda step, lengths: (0,) * len(shape))
    return pl.pallas_call(
        attention_kernel,
        grid_spec=pltpu.PrefetchScalarGridSpec(
            num_scalar_prefetch=1,
            grid=(seq_count // SEQ_STEP,),
            in_specs=[
                whole(seq_count, heads, nope),
                whole(seq_count, heads, rope),
                whole(seq_count, latent),
                whole(seq_count, rope),
                whole(heads * nope, latent),
                pl.BlockSpec((SEQ_STEP, context, latent), lambda step, lengths: (step, 0, 0)),
                pl.BlockSpec((SEQ_STEP, rope, context), lambda step, lengths: (step, 0, 0)),
            ],
            out_specs=pl.BlockSpec((SEQ_STEP, heads, latent), lambda step, lengths: (step, 0, 0)),
            scratch_shapes=[
                pltpu.VMEM((seq_count, heads, latent), jnp.bfloat16),
                pltpu.VMEM((seq_count, heads, rope), jnp.bfloat16),
                pltpu.VMEM((seq_count, 1, latent), jnp.float32),
                pltpu.VMEM((seq_count, 1, rope), jnp.float32),
            ],
        ),
        out_shape=jax.ShapeDtypeStruct((seq_count, heads, latent), jnp.bfloat16),
        compiler_params=pltpu.CompilerParams(dimension_semantics=("arbitrary",), vmem_limit_bytes=60 * 1024 * 1024),
        cost_estimate=pl.CostEstimate(
            flops=8 * seq_count * heads * context * latent,
            bytes_accessed=2 * seq_count * context * (latent + rope),
            transcendentals=seq_count * heads * context,
        ),
        name="attended",
    )(
        lengths, query_nope, query_rope, new_latent, new_rope, absorb, cache_latent, rope_turned
    )


def attention(
    query_nope,
    query_rope,
    new_latent,
    new_rope,
    cache_latent,
    cache_rope,
    lengths,
    absorb_key,
    value_up,
):
    latent_out = attended(
        query_nope, query_rope, new_latent, new_rope, cache_latent, cache_rope, lengths, absorb_key
    )
    return (
        jnp.einsum("shc,chv->shv", latent_out, value_up, preferred_element_type=jnp.float32)
        .astype(jnp.bfloat16)
        .reshape(latent_out.shape[0], -1)
    )


def spread_kernel(
    place_ref,
    pieces_ref,
    own_hidden_ref,
    other_hidden_ref,
    gain_mix_ref,
    gain_in_ref,
    routes_ref,
    outgoing_ref,
    ffn_ref,
    mix_ref,
    taken_ref,
):
    core, block_i, block_j = place_ref[0], place_ref[1], place_ref[2]
    half = own_hidden_ref.shape[0]
    rows = 2 * half
    piece = pieces_ref.shape[-1]
    run = piece // 4
    chunks = []
    for block_row in range(4):
        for i in range(2):
            runs = [
                pieces_ref[
                    c,
                    (i ^ block_i) * 2 + (j ^ block_j),
                    :,
                    block_row * run : (block_row + 1) * run,
                ]
                for j in range(2)
                for c in range(2)
            ]
            chunks.append(jnp.concatenate(runs, axis=-1))
    joined = jnp.concatenate(chunks, axis=0)
    source = lax.broadcasted_iota(jnp.int32, (piece, piece), 0)
    target = lax.broadcasted_iota(jnp.int32, (piece, piece), 1)
    k = run // 4
    goes_to = (source % run) // k * run + source // run * k + source % k
    order = jnp.where(goes_to == target, 1.0, 0.0).astype(jnp.bfloat16)
    placed = jnp.dot(joined, order, preferred_element_type=jnp.float32)
    mixed = jnp.concatenate(
        [placed[n * rows : (n + 1) * rows] for n in range(len(chunks))], axis=-1
    )
    own_hidden = own_hidden_ref[...].astype(jnp.float32)
    other_hidden = other_hidden_ref[...].astype(jnp.float32)
    hidden = jnp.concatenate(
        [
            jnp.where(core == 0, own_hidden, other_hidden),
            jnp.where(core == 0, other_hidden, own_hidden),
        ],
        axis=0,
    )
    after_mix = (
        hidden
        + gain_mix_ref[...].astype(jnp.float32)[None] * normalize(mixed)
    ).astype(jnp.bfloat16)
    after_wide = after_mix.astype(jnp.float32)
    ffn_in = (normalize(after_wide) * gain_in_ref[...].astype(jnp.float32)[None]).astype(jnp.bfloat16)
    ffn_ref[...] = ffn_in
    mix_ref[...] = jnp.where(core == 0, after_wide[:half], after_wide[half:]).astype(jnp.bfloat16)
    slots = taken_ref.shape[0]
    slot = lax.broadcasted_iota(jnp.int32, (slots, rows), 0)
    expert = slot // 2 * 2 + core
    named = jnp.zeros((slots, rows), jnp.float32)
    for n in range(routes_ref.shape[0]):
        named = jnp.where(routes_ref[n : n + 1, :] == expert, 1.0, named)
    earlier = jnp.where(
        lax.broadcasted_iota(jnp.int32, (rows, rows), 0)
        < lax.broadcasted_iota(jnp.int32, (rows, rows), 1),
        1.0,
        0.0,
    ).astype(jnp.bfloat16)
    before = jnp.dot(named.astype(jnp.bfloat16), earlier, preferred_element_type=jnp.float32)
    taken = jnp.where(before == (slot % 2).astype(jnp.float32), named, 0.0).astype(jnp.bfloat16)
    taken_ref[...] = taken
    outgoing = jnp.dot(taken, ffn_in, preferred_element_type=jnp.float32).astype(jnp.bfloat16)
    outgoing_ref[...] = outgoing.reshape(outgoing_ref.shape)


def spread(place, pieces, own_hidden, other_hidden, gain_mix, gain_in, routes, slots):
    rows, width = 2 * own_hidden.shape[0], own_hidden.shape[1]
    return pl.pallas_call(
        spread_kernel,
        in_specs=[pl.BlockSpec(memory_space=pltpu.SMEM)]
        + [pl.BlockSpec(memory_space=pltpu.VMEM)] * 6,
        out_specs=[pl.BlockSpec(memory_space=pltpu.VMEM)] * 4,
        out_shape=[
            jax.ShapeDtypeStruct((slots // 2, 2, width), jnp.bfloat16),
            jax.ShapeDtypeStruct((rows, width), jnp.bfloat16),
            jax.ShapeDtypeStruct((rows // 2, width), jnp.bfloat16),
            jax.ShapeDtypeStruct((slots, rows), jnp.bfloat16),
        ],
        compiler_params=pltpu.CompilerParams(vmem_limit_bytes=8 << 20),
        name="spread",
    )(place, pieces, own_hidden, other_hidden, gain_mix, gain_in, routes.T)


def experts_kernel(rows_ref, gate_ref, up_ref, down_ref, out_ref):
    rows = rows_ref[...].reshape(-1, rows_ref.shape[-1])
    gate_part = jnp.dot(rows, gate_ref[...], preferred_element_type=jnp.float32)
    up_part = jnp.dot(rows, up_ref[...], preferred_element_type=jnp.float32)
    inner = (gate_part / (1.0 + jnp.exp(-gate_part)) * up_part).astype(jnp.bfloat16)
    out = jnp.dot(inner, down_ref[...], preferred_element_type=jnp.float32)
    out_ref[...] = out.astype(out_ref.dtype).reshape(out_ref.shape)


def expert_rows(rows, gate_w, up_w, down_w):
    return pl.pallas_call(
        experts_kernel,
        in_specs=[pl.BlockSpec(memory_space=pltpu.VMEM)] * 4,
        out_specs=pl.BlockSpec(memory_space=pltpu.VMEM),
        out_shape=jax.ShapeDtypeStruct(rows.shape, jnp.bfloat16),
        compiler_params=pltpu.CompilerParams(vmem_limit_bytes=10 << 20),
    )(rows, gate_w, up_w, down_w)


def gathered_kernel(place_ref, weights_ref, returned_ref, shared_ref, kept_ref, given_ref):
    core = place_ref[0]
    rows = weights_ref.shape[0] // 2
    half = rows // 2
    returned = returned_ref[...].reshape(-1, returned_ref.shape[-1])
    both = jnp.dot(weights_ref[...], returned, preferred_element_type=jnp.float32)
    routed = both[:rows] + both[rows:]
    first, second = routed[:half], routed[half:]
    shared = shared_ref[...].astype(jnp.float32)
    kept_ref[...] = jnp.where(core == 0, first, second) + shared
    given_ref[...] = jnp.where(core == 0, second, first)


def gathered(place, weights, returned, shared):
    shape = jax.ShapeDtypeStruct(shared.shape, jnp.float32)
    return pl.pallas_call(
        gathered_kernel,
        in_specs=[pl.BlockSpec(memory_space=pltpu.SMEM)]
        + [pl.BlockSpec(memory_space=pltpu.VMEM)] * 3,
        out_specs=[pl.BlockSpec(memory_space=pltpu.VMEM)] * 2,
        out_shape=[shape, shape],
        compiler_params=pltpu.CompilerParams(vmem_limit_bytes=8 << 20),
        name="gathered",
    )(place, weights, returned, shared)


def routed_kernel(
    rows_hbm,
    gate_hbm,
    up_hbm,
    down_hbm,
    out_ref,
    rows_ref,
    gate_ref,
    up_ref,
    down_ref,
    arrived,
):
    moves = [
        pltpu.make_async_copy(source, target, arrived.at[n])
        for n, (source, target) in enumerate(
            (
                (rows_hbm, rows_ref),
                (gate_hbm, gate_ref),
                (up_hbm, up_ref),
                (down_hbm, down_ref),
            )
        )
    ]
    for move in moves:
        move.start()
    moves[0].wait()
    rows = rows_ref[...].reshape(-1, rows_ref.shape[-1])
    moves[1].wait()
    gate_part = jnp.dot(rows, gate_ref[...], preferred_element_type=jnp.float32)
    moves[2].wait()
    up_part = jnp.dot(rows, up_ref[...], preferred_element_type=jnp.float32)
    inner = (gate_part / (1.0 + jnp.exp(-gate_part)) * up_part).astype(jnp.bfloat16)
    moves[3].wait()
    out = jnp.dot(inner, down_ref[...], preferred_element_type=jnp.float32)
    out_ref[...] = out.astype(out_ref.dtype).reshape(out_ref.shape)


def routed_rows(rows, gate_w, up_w, down_w):
    return pl.pallas_call(
        routed_kernel,
        in_specs=[pl.BlockSpec(memory_space=pltpu.HBM)] * 4,
        out_specs=pl.BlockSpec(memory_space=pltpu.VMEM),
        out_shape=jax.ShapeDtypeStruct(rows.shape, jnp.bfloat16),
        scratch_shapes=[pltpu.VMEM(w.shape, w.dtype) for w in (rows, gate_w, up_w, down_w)]
        + [pltpu.SemaphoreType.DMA((4,))],
        compiler_params=pltpu.CompilerParams(vmem_limit_bytes=64300 << 10),
        name="routed",
    )(rows, gate_w, up_w, down_w)


def local(
    hidden_in,
    query_nope,
    query_rope,
    new_latent,
    new_rope,
    cache_latent,
    cache_rope,
    lengths,
    absorb_key,
    value_up,
    out_proj,
    gain_mix,
    gain_ffn_in,
    router,
    routes,
    expert_gate,
    expert_up,
    expert_down,
    shared_gate,
    shared_up,
    shared_down,
    gain_ffn_out,
):
    seq_count, _ = hidden_in.shape
    core = lax.axis_index("tp")
    own_start = core * seq_count
    slab = sent_to_all(out_proj.T, PLACES).reshape(-1, out_proj.shape[0])
    other_hidden = from_other_core(hidden_in)
    heads_out = attention(
        query_nope,
        query_rope,
        new_latent,
        new_rope,
        cache_latent,
        cache_rope,
        lengths,
        absorb_key,
        value_up,
    )
    chip_heads = lax.all_gather(heads_out, "tp", axis=0, tiled=True)
    block_heads = jnp.concatenate(
        [chip_heads] + [from_partner(chip_heads, flip) for flip in range(1, 4)], axis=0
    )
    partial = lax.dot_general(
        block_heads, slab, (((1,), (1,)), ((), ())), preferred_element_type=jnp.float32
    ).astype(jnp.bfloat16)
    chip_rows = partial.reshape(4, 2 * seq_count, -1)
    pieces = jnp.stack(
        [chip_rows[0]] + [from_partner(chip_rows[flip], flip) for flip in range(1, 4)]
    )
    pieces = lax.all_gather(pieces, "tp", axis=0)
    place = jnp.stack([core, lax.axis_index("ep_0") % 2, lax.axis_index("ep_1") % 2])
    place = place.astype(jnp.int32)
    experts_total = router.shape[1]
    group_rows, top_count = routes.shape
    ep_count = lax.axis_size(EP)
    capacity = 2 * ((group_rows * top_count + experts_total - 1) // experts_total)
    slots = ep_count * capacity
    slot_expert = lax.iota(jnp.int32, slots) // capacity * 2 + core
    outgoing, ffn_in, own_mix, taken = spread(
        place, pieces, hidden_in, other_hidden, gain_mix, gain_ffn_in, routes, slots
    )
    received = lax.all_to_all(
        outgoing, EP, split_axis=0, concat_axis=0, tiled=True
    )
    affinity = jax.nn.sigmoid(jnp.dot(ffn_in, router, preferred_element_type=jnp.float32))
    choose = routes[..., None] == lax.iota(jnp.int32, experts_total)[None, None, :]
    chosen = jnp.sum(jnp.where(choose, affinity[:, None, :], 0.0), axis=-1)
    route_weights = chosen / jnp.sum(chosen, axis=-1, keepdims=True) * routed_scale
    slot_weights = jnp.sum(
        jnp.where(
            routes[:, :, None] == slot_expert[None, None, :], route_weights[:, :, None], 0.0
        ),
        axis=1,
    )
    slot_weights = slot_weights * taken.T.astype(jnp.float32)
    weights_high = slot_weights.astype(jnp.bfloat16)
    weights_low = (slot_weights - weights_high.astype(jnp.float32)).astype(jnp.bfloat16)
    own_ffn = lax.dynamic_slice_in_dim(ffn_in, own_start, seq_count, 0)
    shared = expert_rows(own_ffn, shared_gate, shared_up, shared_down)
    outputs = routed_rows(received, expert_gate[0], expert_up[0], expert_down[0])
    returned = lax.all_to_all(outputs, EP, split_axis=0, concat_axis=0, tiled=True)
    weights = jnp.concatenate([weights_high, weights_low], axis=0)
    kept, given = gathered(place, weights, returned, shared)
    combined = kept + from_other_core(given)
    return (
        own_mix.astype(jnp.float32) + gain_ffn_out.astype(jnp.float32) * normalize(combined)
    ).astype(jnp.bfloat16)


def solution(mesh):
    torus = Mesh(
        mesh.devices.reshape(mesh.shape["grp"], 8, 8, mesh.shape["tp"]),
        ("grp", "ep_0", "ep_1", "tp"),
    )
    in_specs = (
        P(GRP_EP_TP, None),
        P(GRP_EP_TP, None, None),
        P(GRP_EP_TP, None, None),
        P(GRP_EP_TP, None),
        P(GRP_EP_TP, None),
        P(GRP_EP_TP, None, None),
        P(GRP_EP_TP, None, None),
        P(GRP_EP_TP),
        P(),
        P(),
        P(None, EP_TP),
        P(),
        P(),
        P(),
        P(GRP_EP, None),
        P(EP_TP, None, None),
        P(EP_TP, None, None),
        P(EP_TP, None, None),
        P(),
        P(),
        P(),
        P(),
    )
    out_specs = P(GRP_EP_TP, None)

    return jax.shard_map(local, mesh=torus, in_specs=in_specs, out_specs=out_specs, check_vma=False)
```

```python
import math

import jax
import jax.numpy as jnp
from jax import lax
from jax.experimental import pallas as pl
from jax.experimental.pallas import tpu as pltpu
from jax.sharding import Mesh
from jax.sharding import PartitionSpec as P

SEQ_STEP = 4
EP = ("ep_0", "ep_1")
GRP_EP_TP = ("grp", "ep_0", "ep_1", "tp")
EP_TP = ("ep_0", "ep_1", "tp")
GRP_EP = ("grp", "ep_0", "ep_1")


rope_theta = 10000.0
norm_eps = 1e-06
routed_scale = 2.5
masked_score = -1e30


def device_at(row, col, core):
    return (row * 8 + col) * 2 + core


COLUMN_GROUPS = [[device_at(row, col, core) for col in range(8) for core in range(2)] for row in range(8)]
BLOCKS = [
    [device_at(row, 2 * pair + col, core) for row in range(8) for col in range(2)]
    for pair in range(4)
    for core in range(2)
]
HALVES = 2
QUARTERS = 4


def repeat_kernel(array_ref, out_ref):
    run = out_ref.shape[-1]
    count = array_ref.shape[-1] // run
    for n in range(out_ref.shape[0]):
        out_ref[n] = array_ref[:, n % count * run : (n % count + 1) * run]


def in_parts(array, count, times):
    rows, width = array.shape
    return pl.pallas_call(
        repeat_kernel,
        in_specs=[pl.BlockSpec(memory_space=pltpu.VMEM)],
        out_specs=pl.BlockSpec(memory_space=pltpu.VMEM),
        out_shape=jax.ShapeDtypeStruct((count * times, rows, width // count), array.dtype),
        compiler_params=pltpu.CompilerParams(vmem_limit_bytes=4 << 20),
        name="parts",
    )(array)


def project_kernel(place_ref, heads_ref, own_slab_ref, other_slab_ref, out_ref):
    core = place_ref[0]
    heads = heads_ref[...].reshape(-1, heads_ref.shape[-1])
    run = own_slab_ref.shape[-1]
    first, second = heads[:, :run], heads[:, run:]
    own = jnp.where(core == 0, first, second)
    other = jnp.where(core == 0, second, first)
    dims = (((1,), (1,)), ((), ()))
    out = lax.dot_general(
        own, own_slab_ref[...], dims, preferred_element_type=jnp.float32
    ) + lax.dot_general(other, other_slab_ref[...], dims, preferred_element_type=jnp.float32)
    out_ref[...] = out.astype(jnp.bfloat16).reshape(out_ref.shape)


def projected(place, heads, own_slab, other_slab):
    return pl.pallas_call(
        project_kernel,
        in_specs=[pl.BlockSpec(memory_space=pltpu.SMEM)]
        + [pl.BlockSpec(memory_space=pltpu.VMEM)] * 3,
        out_specs=pl.BlockSpec(memory_space=pltpu.VMEM),
        out_shape=jax.ShapeDtypeStruct((*heads.shape[:2], own_slab.shape[0]), jnp.bfloat16),
        compiler_params=pltpu.CompilerParams(vmem_limit_bytes=6 << 20),
        name="projected",
    )(place, heads, own_slab, other_slab)


def exchanged(blocks, groups):
    return lax.all_to_all(blocks, EP_TP, 0, 0, axis_index_groups=groups, tiled=True)


def from_other_core(array):
    return lax.ppermute(array, "tp", [(0, 1), (1, 0)])


def normalize(values):
    return values * lax.rsqrt(jnp.mean(values * values, axis=-1, keepdims=True) + norm_eps)


def attention_kernel(
    lengths_ref,
    nope_ref,
    rope_ref,
    latent_ref,
    key_ref,
    absorb_ref,
    cache_ref,
    cache_rope_ref,
    out_ref,
    query_ref,
    query_pe_ref,
    latent_new_ref,
    key_new_ref,
):
    step = pl.program_id(0)
    seq_count, heads, nope = nope_ref.shape
    rope = rope_ref.shape[-1]
    half = rope // 2
    latent = cache_ref.shape[-1]
    scale = (nope + rope) ** (-0.5)

    def turned(values, cosine, sine):
        swapped = jnp.concatenate([values[..., half:], values[..., :half]], axis=-1)
        return values * cosine + swapped * sine

    @pl.when(step == 0)
    def _():
        rows = nope_ref[...].reshape(seq_count * heads, nope)
        twice = jnp.concatenate([rows, rows], axis=-1)
        wide = jnp.concatenate([twice] * (heads // 2), axis=-1)
        row_head = lax.broadcasted_iota(jnp.int32, wide.shape, 0) % heads
        column_head = lax.broadcasted_iota(jnp.int32, wide.shape, 1) // nope
        wide = jnp.where(row_head == column_head, wide.astype(jnp.float32), 0.0)
        queries = jnp.dot(
            wide.astype(jnp.bfloat16), absorb_ref[...], preferred_element_type=jnp.float32
        )
        query_ref[...] = queries.reshape(seq_count, heads, latent).astype(jnp.bfloat16)
        row = lax.broadcasted_iota(jnp.int32, (seq_count, rope), 0)
        column = lax.broadcasted_iota(jnp.int32, (seq_count, rope), 1)
        position = jnp.zeros((seq_count, rope), jnp.int32)
        for n in range(seq_count):
            position = jnp.where(row == n, lengths_ref[n], position)
        exponent = (column % half).astype(jnp.float32) * (-2.0 / rope * math.log(rope_theta))
        angles = position.astype(jnp.float32) * jnp.exp(exponent)
        cosine = jnp.cos(angles)
        sine = jnp.sin(angles)
        sine = jnp.where(column < half, -sine, sine)
        query_pe_ref[...] = turned(
            rope_ref[...].astype(jnp.float32), cosine[:, None, :], sine[:, None, :]
        ).astype(jnp.bfloat16)
        latent_new = normalize(latent_ref[...].astype(jnp.float32)).astype(jnp.bfloat16)
        latent_new_ref[...] = latent_new.astype(jnp.float32)[:, None, :]
        key_new = turned(key_ref[...].astype(jnp.float32), cosine, sine)
        key_new_ref[...] = key_new.astype(jnp.bfloat16).astype(jnp.float32)[:, None, :]

    places = range(cache_ref.shape[0])
    seqs = [step * cache_ref.shape[0] + place for place in places]
    rows = cache_ref.shape[0] * heads
    query = query_ref[pl.ds(step * cache_ref.shape[0], cache_ref.shape[0])]
    query_pe = query_pe_ref[pl.ds(step * cache_ref.shape[0], cache_ref.shape[0])]
    latent_wide = latent_new_ref[pl.ds(step * cache_ref.shape[0], cache_ref.shape[0])]
    key_wide = key_new_ref[pl.ds(step * cache_ref.shape[0], cache_ref.shape[0])]
    score_new = (
        jnp.sum(query.astype(jnp.float32) * latent_wide, axis=-1, keepdims=True)
        + jnp.sum(query_pe.astype(jnp.float32) * key_wide, axis=-1, keepdims=True)
    ).reshape(rows, 1) * scale
    parts = [
        lax.dot_general(
            query[place], cache_ref[place], (((1,), (1,)), ((), ())),
            preferred_element_type=jnp.float32,
        )
        + jnp.dot(query_pe[place], cache_rope_ref[place], preferred_element_type=jnp.float32)
        for place in places
    ]
    position = lax.broadcasted_iota(jnp.int32, parts[0].shape, 1)
    scores = jnp.concatenate(
        [
            jnp.where(position < lengths_ref[seq], part * scale, masked_score)
            for seq, part in zip(seqs, parts)
        ],
        axis=0,
    )
    row_max = jnp.maximum(jnp.max(scores, axis=-1, keepdims=True), score_new)
    weights = jnp.exp(scores - row_max)
    weight_new = jnp.exp(score_new - row_max)
    total = jnp.sum(weights, axis=-1, keepdims=True) + weight_new
    rounded = weights.astype(jnp.bfloat16)
    summed = jnp.concatenate(
        [
            jnp.dot(
                rounded[place * heads : (place + 1) * heads],
                cache_ref[place],
                preferred_element_type=jnp.float32,
            )
            for place in places
        ],
        axis=0,
    )
    fresh = jnp.broadcast_to(latent_wide, query.shape).reshape(rows, latent)
    summed = summed + weight_new.astype(jnp.bfloat16).astype(jnp.float32) * fresh
    out_ref[...] = (summed / total).astype(jnp.bfloat16).reshape(out_ref.shape)


def attended(query_nope, query_rope, new_latent, new_rope, cache_latent, cache_rope, lengths, absorb_key):
    seq_count, heads, nope = query_nope.shape
    rope = query_rope.shape[-1]
    latent = cache_latent.shape[-1]
    context = cache_latent.shape[1]
    absorb = absorb_key.transpose(1, 2, 0).reshape(heads * nope, latent)
    rope_turned = cache_rope.transpose(0, 2, 1)
    whole = lambda *shape: pl.BlockSpec(shape, lambda step, lengths: (0,) * len(shape))
    return pl.pallas_call(
        attention_kernel,
        grid_spec=pltpu.PrefetchScalarGridSpec(
            num_scalar_prefetch=1,
            grid=(seq_count // SEQ_STEP,),
            in_specs=[
                whole(seq_count, heads, nope),
                whole(seq_count, heads, rope),
                whole(seq_count, latent),
                whole(seq_count, rope),
                whole(heads * nope, latent),
                pl.BlockSpec((SEQ_STEP, context, latent), lambda step, lengths: (step, 0, 0)),
                pl.BlockSpec((SEQ_STEP, rope, context), lambda step, lengths: (step, 0, 0)),
            ],
            out_specs=pl.BlockSpec((SEQ_STEP, heads, latent), lambda step, lengths: (step, 0, 0)),
            scratch_shapes=[
                pltpu.VMEM((seq_count, heads, latent), jnp.bfloat16),
                pltpu.VMEM((seq_count, heads, rope), jnp.bfloat16),
                pltpu.VMEM((seq_count, 1, latent), jnp.float32),
                pltpu.VMEM((seq_count, 1, rope), jnp.float32),
            ],
        ),
        out_shape=jax.ShapeDtypeStruct((seq_count, heads, latent), jnp.bfloat16),
        compiler_params=pltpu.CompilerParams(dimension_semantics=("arbitrary",), vmem_limit_bytes=60 * 1024 * 1024),
        cost_estimate=pl.CostEstimate(
            flops=8 * seq_count * heads * context * latent,
            bytes_accessed=2 * seq_count * context * (latent + rope),
            transcendentals=seq_count * heads * context,
        ),
        name="attended",
    )(
        lengths, query_nope, query_rope, new_latent, new_rope, absorb, cache_latent, rope_turned
    )


def attention(
    query_nope,
    query_rope,
    new_latent,
    new_rope,
    cache_latent,
    cache_rope,
    lengths,
    absorb_key,
    value_up,
):
    latent_out = attended(
        query_nope, query_rope, new_latent, new_rope, cache_latent, cache_rope, lengths, absorb_key
    )
    return (
        jnp.einsum("shc,chv->shv", latent_out, value_up, preferred_element_type=jnp.float32)
        .astype(jnp.bfloat16)
        .reshape(latent_out.shape[0], -1)
    )


def spread_kernel(
    place_ref,
    own_pieces_ref,
    other_pieces_ref,
    own_hidden_ref,
    other_hidden_ref,
    gain_mix_ref,
    gain_in_ref,
    routes_ref,
    outgoing_ref,
    ffn_ref,
    mix_ref,
    taken_ref,
):
    core = place_ref[0]
    half = own_hidden_ref.shape[0]
    rows = 2 * half

    def in_columns(pieces_ref):
        parts = [
            pieces_ref[HALVES * n].astype(jnp.float32) + pieces_ref[HALVES * n + 1].astype(jnp.float32)
            for n in range(pieces_ref.shape[0] // HALVES)
        ]
        return jnp.concatenate(parts, axis=-1)

    own_mixed = in_columns(own_pieces_ref)
    other_mixed = in_columns(other_pieces_ref)
    mixed = jnp.concatenate(
        [
            jnp.where(core == 0, own_mixed, other_mixed),
            jnp.where(core == 0, other_mixed, own_mixed),
        ],
        axis=0,
    )
    mixed = mixed.astype(jnp.bfloat16).astype(jnp.float32)
    own_hidden = own_hidden_ref[...].astype(jnp.float32)
    other_hidden = other_hidden_ref[...].astype(jnp.float32)
    hidden = jnp.concatenate(
        [
            jnp.where(core == 0, own_hidden, other_hidden),
            jnp.where(core == 0, other_hidden, own_hidden),
        ],
        axis=0,
    )
    after_mix = (
        hidden
        + gain_mix_ref[...].astype(jnp.float32)[None] * normalize(mixed)
    ).astype(jnp.bfloat16)
    after_wide = after_mix.astype(jnp.float32)
    ffn_in = (normalize(after_wide) * gain_in_ref[...].astype(jnp.float32)[None]).astype(jnp.bfloat16)
    ffn_ref[...] = ffn_in
    mix_ref[...] = jnp.where(core == 0, after_wide[:half], after_wide[half:]).astype(jnp.bfloat16)
    slots = taken_ref.shape[0]
    slot = lax.broadcasted_iota(jnp.int32, (slots, rows), 0)
    expert = slot // 2 * 2 + core
    named = jnp.zeros((slots, rows), jnp.float32)
    for n in range(routes_ref.shape[0]):
        named = jnp.where(routes_ref[n : n + 1, :] == expert, 1.0, named)
    earlier = jnp.where(
        lax.broadcasted_iota(jnp.int32, (rows, rows), 0)
        < lax.broadcasted_iota(jnp.int32, (rows, rows), 1),
        1.0,
        0.0,
    ).astype(jnp.bfloat16)
    before = jnp.dot(named.astype(jnp.bfloat16), earlier, preferred_element_type=jnp.float32)
    taken = jnp.where(before == (slot % 2).astype(jnp.float32), named, 0.0).astype(jnp.bfloat16)
    taken_ref[...] = taken
    outgoing = jnp.dot(taken, ffn_in, preferred_element_type=jnp.float32).astype(jnp.bfloat16)
    outgoing_ref[...] = outgoing.reshape(outgoing_ref.shape)


def spread(place, own_pieces, other_pieces, own_hidden, other_hidden, gain_mix, gain_in, routes, slots):
    rows, width = 2 * own_hidden.shape[0], own_hidden.shape[1]
    return pl.pallas_call(
        spread_kernel,
        in_specs=[pl.BlockSpec(memory_space=pltpu.SMEM)]
        + [pl.BlockSpec(memory_space=pltpu.VMEM)] * 7,
        out_specs=[pl.BlockSpec(memory_space=pltpu.VMEM)] * 4,
        out_shape=[
            jax.ShapeDtypeStruct((slots // 2, 2, width), jnp.bfloat16),
            jax.ShapeDtypeStruct((rows, width), jnp.bfloat16),
            jax.ShapeDtypeStruct((rows // 2, width), jnp.bfloat16),
            jax.ShapeDtypeStruct((slots, rows), jnp.bfloat16),
        ],
        compiler_params=pltpu.CompilerParams(vmem_limit_bytes=8 << 20),
        name="spread",
    )(
        place,
        own_pieces,
        other_pieces,
        own_hidden,
        other_hidden,
        gain_mix,
        gain_in,
        routes.T,
    )


def experts_kernel(rows_ref, gate_ref, up_ref, down_ref, out_ref):
    rows = rows_ref[...].reshape(-1, rows_ref.shape[-1])
    gate_part = jnp.dot(rows, gate_ref[...], preferred_element_type=jnp.float32)
    up_part = jnp.dot(rows, up_ref[...], preferred_element_type=jnp.float32)
    inner = (gate_part / (1.0 + jnp.exp(-gate_part)) * up_part).astype(jnp.bfloat16)
    out = jnp.dot(inner, down_ref[...], preferred_element_type=jnp.float32)
    out_ref[...] = out.astype(out_ref.dtype).reshape(out_ref.shape)


def expert_rows(rows, gate_w, up_w, down_w):
    return pl.pallas_call(
        experts_kernel,
        in_specs=[pl.BlockSpec(memory_space=pltpu.VMEM)] * 4,
        out_specs=pl.BlockSpec(memory_space=pltpu.VMEM),
        out_shape=jax.ShapeDtypeStruct(rows.shape, jnp.bfloat16),
        compiler_params=pltpu.CompilerParams(vmem_limit_bytes=10 << 20),
    )(rows, gate_w, up_w, down_w)


def gathered_kernel(place_ref, weights_ref, returned_ref, shared_ref, kept_ref, given_ref):
    core = place_ref[0]
    rows = weights_ref.shape[0] // 2
    half = rows // 2
    returned = returned_ref[...].reshape(-1, returned_ref.shape[-1])
    both = jnp.dot(weights_ref[...], returned, preferred_element_type=jnp.float32)
    routed = both[:rows] + both[rows:]
    first, second = routed[:half], routed[half:]
    shared = shared_ref[...].astype(jnp.float32)
    kept_ref[...] = jnp.where(core == 0, first, second) + shared
    given_ref[...] = jnp.where(core == 0, second, first)


def gathered(place, weights, returned, shared):
    shape = jax.ShapeDtypeStruct(shared.shape, jnp.float32)
    return pl.pallas_call(
        gathered_kernel,
        in_specs=[pl.BlockSpec(memory_space=pltpu.SMEM)]
        + [pl.BlockSpec(memory_space=pltpu.VMEM)] * 3,
        out_specs=[pl.BlockSpec(memory_space=pltpu.VMEM)] * 2,
        out_shape=[shape, shape],
        compiler_params=pltpu.CompilerParams(vmem_limit_bytes=8 << 20),
        name="gathered",
    )(place, weights, returned, shared)


def routed_kernel(
    rows_hbm,
    gate_hbm,
    up_hbm,
    down_hbm,
    out_ref,
    rows_ref,
    gate_ref,
    up_ref,
    down_ref,
    arrived,
):
    moves = [
        pltpu.make_async_copy(source, target, arrived.at[n])
        for n, (source, target) in enumerate(
            (
                (rows_hbm, rows_ref),
                (gate_hbm, gate_ref),
                (up_hbm, up_ref),
                (down_hbm, down_ref),
            )
        )
    ]
    for move in moves:
        move.start()
    moves[0].wait()
    rows = rows_ref[...].reshape(-1, rows_ref.shape[-1])
    moves[1].wait()
    gate_part = jnp.dot(rows, gate_ref[...], preferred_element_type=jnp.float32)
    moves[2].wait()
    up_part = jnp.dot(rows, up_ref[...], preferred_element_type=jnp.float32)
    inner = (gate_part / (1.0 + jnp.exp(-gate_part)) * up_part).astype(jnp.bfloat16)
    moves[3].wait()
    out = jnp.dot(inner, down_ref[...], preferred_element_type=jnp.float32)
    out_ref[...] = out.astype(out_ref.dtype).reshape(out_ref.shape)


def routed_rows(rows, gate_w, up_w, down_w):
    return pl.pallas_call(
        routed_kernel,
        in_specs=[pl.BlockSpec(memory_space=pltpu.HBM)] * 4,
        out_specs=pl.BlockSpec(memory_space=pltpu.VMEM),
        out_shape=jax.ShapeDtypeStruct(rows.shape, jnp.bfloat16),
        scratch_shapes=[pltpu.VMEM(w.shape, w.dtype) for w in (rows, gate_w, up_w, down_w)]
        + [pltpu.SemaphoreType.DMA((4,))],
        compiler_params=pltpu.CompilerParams(vmem_limit_bytes=64300 << 10),
        name="routed",
    )(rows, gate_w, up_w, down_w)


def local(
    hidden_in,
    query_nope,
    query_rope,
    new_latent,
    new_rope,
    cache_latent,
    cache_rope,
    lengths,
    absorb_key,
    value_up,
    out_proj,
    gain_mix,
    gain_ffn_in,
    router,
    routes,
    expert_gate,
    expert_up,
    expert_down,
    shared_gate,
    shared_up,
    shared_down,
    gain_ffn_out,
):
    seq_count, _ = hidden_in.shape
    core = lax.axis_index("tp")
    own_start = core * seq_count
    place = core[None].astype(jnp.int32)
    quarters = in_parts(out_proj.T, QUARTERS, len(COLUMN_GROUPS[0]) // QUARTERS)
    slab = exchanged(quarters, COLUMN_GROUPS).reshape(-1, quarters.shape[-1])
    other_slab = from_other_core(slab)
    other_hidden = from_other_core(hidden_in)
    heads_out = attention(
        query_nope,
        query_rope,
        new_latent,
        new_rope,
        cache_latent,
        cache_rope,
        lengths,
        absorb_key,
        value_up,
    )
    block_heads = exchanged(in_parts(heads_out, HALVES, len(BLOCKS[0]) // HALVES), BLOCKS)
    partial = projected(place, block_heads, slab, other_slab)
    pieces = exchanged(partial, BLOCKS)
    other_pieces = from_other_core(pieces)
    experts_total = router.shape[1]
    group_rows, top_count = routes.shape
    ep_count = lax.axis_size(EP)
    capacity = 2 * ((group_rows * top_count + experts_total - 1) // experts_total)
    slots = ep_count * capacity
    slot_expert = lax.iota(jnp.int32, slots) // capacity * 2 + core
    outgoing, ffn_in, own_mix, taken = spread(
        place,
        pieces,
        other_pieces,
        hidden_in,
        other_hidden,
        gain_mix,
        gain_ffn_in,
        routes,
        slots,
    )
    received = lax.all_to_all(
        outgoing, EP, split_axis=0, concat_axis=0, tiled=True
    )
    affinity = jax.nn.sigmoid(jnp.dot(ffn_in, router, preferred_element_type=jnp.float32))
    choose = routes[..., None] == lax.iota(jnp.int32, experts_total)[None, None, :]
    chosen = jnp.sum(jnp.where(choose, affinity[:, None, :], 0.0), axis=-1)
    route_weights = chosen / jnp.sum(chosen, axis=-1, keepdims=True) * routed_scale
    slot_weights = jnp.sum(
        jnp.where(
            routes[:, :, None] == slot_expert[None, None, :], route_weights[:, :, None], 0.0
        ),
        axis=1,
    )
    slot_weights = slot_weights * taken.T.astype(jnp.float32)
    weights_high = slot_weights.astype(jnp.bfloat16)
    weights_low = (slot_weights - weights_high.astype(jnp.float32)).astype(jnp.bfloat16)
    own_ffn = lax.dynamic_slice_in_dim(ffn_in, own_start, seq_count, 0)
    shared = expert_rows(own_ffn, shared_gate, shared_up, shared_down)
    outputs = routed_rows(received, expert_gate[0], expert_up[0], expert_down[0])
    returned = lax.all_to_all(outputs, EP, split_axis=0, concat_axis=0, tiled=True)
    weights = jnp.concatenate([weights_high, weights_low], axis=0)
    kept, given = gathered(place, weights, returned, shared)
    combined = kept + from_other_core(given)
    return (
        own_mix.astype(jnp.float32) + gain_ffn_out.astype(jnp.float32) * normalize(combined)
    ).astype(jnp.bfloat16)


def solution(mesh):
    torus = Mesh(
        mesh.devices.reshape(mesh.shape["grp"], 8, 8, mesh.shape["tp"]),
        ("grp", "ep_0", "ep_1", "tp"),
    )
    in_specs = (
        P(GRP_EP_TP, None),
        P(GRP_EP_TP, None, None),
        P(GRP_EP_TP, None, None),
        P(GRP_EP_TP, None),
        P(GRP_EP_TP, None),
        P(GRP_EP_TP, None, None),
        P(GRP_EP_TP, None, None),
        P(GRP_EP_TP),
        P(),
        P(),
        P(None, EP_TP),
        P(),
        P(),
        P(),
        P(GRP_EP, None),
        P(EP_TP, None, None),
        P(EP_TP, None, None),
        P(EP_TP, None, None),
        P(),
        P(),
        P(),
        P(),
    )
    out_specs = P(GRP_EP_TP, None)

    return jax.shard_map(local, mesh=torus, in_specs=in_specs, out_specs=out_specs, check_vma=False)
```

```python
import math

import jax
import jax.numpy as jnp
from jax import lax
from jax.experimental import pallas as pl
from jax.experimental.pallas import tpu as pltpu
from jax.sharding import Mesh
from jax.sharding import PartitionSpec as P

SEQ_STEP = 4
OUT_CHUNKS = 4
EP = ("ep_0", "ep_1")
GRP_EP_TP = ("grp", "ep_0", "ep_1", "tp")
EP_TP = ("ep_0", "ep_1", "tp")
GRP_EP = ("grp", "ep_0", "ep_1")


rope_theta = 10000.0
norm_eps = 1e-06
routed_scale = 2.5
masked_score = -1e30


def device_at(row, col, core):
    return (row * 8 + col) * 2 + core


COLUMN_GROUPS = [
    [device_at(row, col, core) for col in range(8)] for row in range(8) for core in range(2)
]
BLOCKS = [
    [device_at(row, 2 * pair + col, core) for row in range(8) for col in range(2)]
    for pair in range(4)
    for core in range(2)
]
HALVES = 2


def repeat_kernel(array_ref, out_ref):
    run = out_ref.shape[-1]
    count = array_ref.shape[-1] // run
    for n in range(out_ref.shape[0]):
        out_ref[n] = array_ref[:, n % count * run : (n % count + 1) * run]


def in_parts(array, count, times):
    rows, width = array.shape
    return pl.pallas_call(
        repeat_kernel,
        in_specs=[pl.BlockSpec(memory_space=pltpu.VMEM)],
        out_specs=pl.BlockSpec(memory_space=pltpu.VMEM),
        out_shape=jax.ShapeDtypeStruct((count * times, rows, width // count), array.dtype),
        compiler_params=pltpu.CompilerParams(vmem_limit_bytes=4 << 20),
        name="parts",
    )(array)


def project_kernel(place_ref, heads_ref, own_slab_ref, other_slab_ref, out_ref):
    core = place_ref[0]
    heads = heads_ref[...].reshape(-1, heads_ref.shape[-1])
    dims = (((1,), (1,)), ((), ()))
    own = lax.dot_general(heads, own_slab_ref[...], dims, preferred_element_type=jnp.float32)
    other = lax.dot_general(heads, other_slab_ref[...], dims, preferred_element_type=jnp.float32)
    joined = jnp.concatenate(
        [jnp.where(core == 0, own, other), jnp.where(core == 0, other, own)], axis=-1
    ).astype(jnp.bfloat16)
    count = joined.shape[-1]
    source = lax.broadcasted_iota(jnp.int32, (count, count), 0)
    target = lax.broadcasted_iota(jnp.int32, (count, count), 1)
    run = count // 16
    goes_to = source % (count // 2) // run * (2 * run) + source // (count // 2) * run + source % run
    order = jnp.where(goes_to == target, 1.0, 0.0).astype(jnp.bfloat16)
    out = jnp.dot(joined, order, preferred_element_type=jnp.float32)
    out_ref[...] = out.astype(jnp.bfloat16).reshape(out_ref.shape)


def projected(place, heads, own_slab, other_slab):
    return pl.pallas_call(
        project_kernel,
        in_specs=[pl.BlockSpec(memory_space=pltpu.SMEM)]
        + [pl.BlockSpec(memory_space=pltpu.VMEM)] * 3,
        out_specs=pl.BlockSpec(memory_space=pltpu.VMEM),
        out_shape=jax.ShapeDtypeStruct((*heads.shape[:2], 2 * own_slab.shape[0]), jnp.bfloat16),
        compiler_params=pltpu.CompilerParams(vmem_limit_bytes=6 << 20),
        name="projected",
    )(place, heads, own_slab, other_slab)


def exchanged(blocks, groups):
    return lax.all_to_all(blocks, EP_TP, 0, 0, axis_index_groups=groups, tiled=True)


def from_other_core(array):
    return lax.ppermute(array, "tp", [(0, 1), (1, 0)])


def normalize(values):
    return values * lax.rsqrt(jnp.mean(values * values, axis=-1, keepdims=True) + norm_eps)


def attention_kernel(
    lengths_ref,
    nope_ref,
    rope_ref,
    latent_ref,
    key_ref,
    absorb_ref,
    cache_hbm,
    cache_rope_hbm,
    out_ref,
    cache_ref,
    cache_rope_ref,
    arrived,
):
    moves = []
    for n in range(cache_ref.shape[0] // SEQ_STEP):
        group = pl.ds(n * SEQ_STEP, SEQ_STEP)
        moves.append(
            (
                pltpu.make_async_copy(cache_hbm.at[group], cache_ref.at[group], arrived.at[n, 0]),
                pltpu.make_async_copy(
                    cache_rope_hbm.at[group], cache_rope_ref.at[group], arrived.at[n, 1]
                ),
            )
        )
    for pair in moves:
        for move in pair:
            move.start()
    seq_count, heads, nope = nope_ref.shape
    rope = rope_ref.shape[-1]
    half = rope // 2
    latent = cache_ref.shape[-1]
    scale = (nope + rope) ** (-0.5)

    def turned(values, cosine, sine):
        swapped = jnp.concatenate([values[..., half:], values[..., :half]], axis=-1)
        return values * cosine + swapped * sine

    rows = nope_ref[...].reshape(seq_count * heads, nope)
    twice = jnp.concatenate([rows, rows], axis=-1)
    wide = jnp.concatenate([twice] * (heads // 2), axis=-1)
    row_head = lax.broadcasted_iota(jnp.int32, wide.shape, 0) % heads
    column_head = lax.broadcasted_iota(jnp.int32, wide.shape, 1) // nope
    wide = jnp.where(row_head == column_head, wide.astype(jnp.float32), 0.0)
    queries = jnp.dot(
        wide.astype(jnp.bfloat16), absorb_ref[...], preferred_element_type=jnp.float32
    )
    query_all = queries.reshape(seq_count, heads, latent).astype(jnp.bfloat16)
    row = lax.broadcasted_iota(jnp.int32, (seq_count, rope), 0)
    column = lax.broadcasted_iota(jnp.int32, (seq_count, rope), 1)
    position = jnp.zeros((seq_count, rope), jnp.int32)
    for n in range(seq_count):
        position = jnp.where(row == n, lengths_ref[n], position)
    exponent = (column % half).astype(jnp.float32) * (-2.0 / rope * math.log(rope_theta))
    angles = position.astype(jnp.float32) * jnp.exp(exponent)
    cosine = jnp.cos(angles)
    sine = jnp.sin(angles)
    sine = jnp.where(column < half, -sine, sine)
    query_pe_all = turned(
        rope_ref[...].astype(jnp.float32), cosine[:, None, :], sine[:, None, :]
    ).astype(jnp.bfloat16)
    latent_new = normalize(latent_ref[...].astype(jnp.float32)).astype(jnp.bfloat16)
    latent_new_all = latent_new.astype(jnp.float32)[:, None, :]
    key_new = turned(key_ref[...].astype(jnp.float32), cosine, sine)
    key_new_all = key_new.astype(jnp.bfloat16).astype(jnp.float32)[:, None, :]

    for step in range(len(moves)):
        places = range(SEQ_STEP)
        seqs = [step * SEQ_STEP + place for place in places]
        rows = SEQ_STEP * heads
        group = slice(step * SEQ_STEP, (step + 1) * SEQ_STEP)
        query = query_all[group]
        query_pe = query_pe_all[group]
        latent_wide = latent_new_all[group]
        key_wide = key_new_all[group]
        for move in moves[step]:
            move.wait()
        score_new = (
            jnp.sum(query.astype(jnp.float32) * latent_wide, axis=-1, keepdims=True)
            + jnp.sum(query_pe.astype(jnp.float32) * key_wide, axis=-1, keepdims=True)
        ).reshape(rows, 1) * scale
        parts = [
            lax.dot_general(
                query[place], cache_ref[seqs[place]], (((1,), (1,)), ((), ())),
                preferred_element_type=jnp.float32,
            )
            + jnp.dot(query_pe[place], cache_rope_ref[seqs[place]], preferred_element_type=jnp.float32)
            for place in places
        ]
        position = lax.broadcasted_iota(jnp.int32, parts[0].shape, 1)
        scores = jnp.concatenate(
            [
                jnp.where(position < lengths_ref[seq], part * scale, masked_score)
                for seq, part in zip(seqs, parts)
            ],
            axis=0,
        )
        row_max = jnp.maximum(jnp.max(scores, axis=-1, keepdims=True), score_new)
        weights = jnp.exp(scores - row_max)
        weight_new = jnp.exp(score_new - row_max)
        total = jnp.sum(weights, axis=-1, keepdims=True) + weight_new
        rounded = weights.astype(jnp.bfloat16)
        summed = jnp.concatenate(
            [
                jnp.dot(
                    rounded[place * heads : (place + 1) * heads],
                    cache_ref[seqs[place]],
                    preferred_element_type=jnp.float32,
                )
                for place in places
            ],
            axis=0,
        )
        fresh = jnp.broadcast_to(latent_wide, query.shape).reshape(rows, latent)
        summed = summed + weight_new.astype(jnp.bfloat16).astype(jnp.float32) * fresh
        out_ref[group] = (summed / total).astype(jnp.bfloat16).reshape(SEQ_STEP, heads, latent)


def attended(query_nope, query_rope, new_latent, new_rope, cache_latent, cache_rope, lengths, absorb_key):
    seq_count, heads, nope = query_nope.shape
    rope = query_rope.shape[-1]
    latent = cache_latent.shape[-1]
    context = cache_latent.shape[1]
    absorb = absorb_key.transpose(1, 2, 0).reshape(heads * nope, latent)
    rope_turned = cache_rope.transpose(0, 2, 1)
    return pl.pallas_call(
        attention_kernel,
        in_specs=[pl.BlockSpec(memory_space=pltpu.SMEM)]
        + [pl.BlockSpec(memory_space=pltpu.VMEM)] * 5
        + [pl.BlockSpec(memory_space=pltpu.HBM)] * 2,
        out_specs=pl.BlockSpec(memory_space=pltpu.VMEM),
        scratch_shapes=[
            pltpu.VMEM(cache_latent.shape, jnp.bfloat16),
            pltpu.VMEM(rope_turned.shape, jnp.bfloat16),
            pltpu.SemaphoreType.DMA((seq_count // SEQ_STEP, 2)),
        ],
        out_shape=jax.ShapeDtypeStruct((seq_count, heads, latent), jnp.bfloat16),
        compiler_params=pltpu.CompilerParams(vmem_limit_bytes=60 * 1024 * 1024),
        cost_estimate=pl.CostEstimate(
            flops=8 * seq_count * heads * context * latent,
            bytes_accessed=2 * seq_count * context * (latent + rope),
            transcendentals=seq_count * heads * context,
        ),
        name="attended",
    )(
        lengths, query_nope, query_rope, new_latent, new_rope, absorb, cache_latent, rope_turned
    )


def attention(
    query_nope,
    query_rope,
    new_latent,
    new_rope,
    cache_latent,
    cache_rope,
    lengths,
    absorb_key,
    value_up,
):
    latent_out = attended(
        query_nope, query_rope, new_latent, new_rope, cache_latent, cache_rope, lengths, absorb_key
    )
    return (
        jnp.einsum("shc,chv->shv", latent_out, value_up, preferred_element_type=jnp.float32)
        .astype(jnp.bfloat16)
        .reshape(latent_out.shape[0], -1)
    )


def spread_kernel(
    place_ref,
    own_pieces_ref,
    other_pieces_ref,
    own_hidden_ref,
    other_hidden_ref,
    gain_mix_ref,
    gain_in_ref,
    routes_ref,
    outgoing_ref,
    ffn_ref,
    mix_ref,
    taken_ref,
):
    core = place_ref[0]
    half = own_hidden_ref.shape[0]
    rows = 2 * half

    def in_columns(pieces_ref):
        parts = [
            pieces_ref[HALVES * n].astype(jnp.float32) + pieces_ref[HALVES * n + 1].astype(jnp.float32)
            for n in range(pieces_ref.shape[0] // HALVES)
        ]
        return jnp.concatenate(parts, axis=-1)

    own_mixed = in_columns(own_pieces_ref)
    other_mixed = in_columns(other_pieces_ref)
    mixed = jnp.concatenate(
        [
            jnp.where(core == 0, own_mixed, other_mixed),
            jnp.where(core == 0, other_mixed, own_mixed),
        ],
        axis=0,
    )
    mixed = mixed.astype(jnp.bfloat16).astype(jnp.float32)
    own_hidden = own_hidden_ref[...].astype(jnp.float32)
    other_hidden = other_hidden_ref[...].astype(jnp.float32)
    hidden = jnp.concatenate(
        [
            jnp.where(core == 0, own_hidden, other_hidden),
            jnp.where(core == 0, other_hidden, own_hidden),
        ],
        axis=0,
    )
    after_mix = (
        hidden
        + gain_mix_ref[...].astype(jnp.float32)[None] * normalize(mixed)
    ).astype(jnp.bfloat16)
    after_wide = after_mix.astype(jnp.float32)
    ffn_in = (normalize(after_wide) * gain_in_ref[...].astype(jnp.float32)[None]).astype(jnp.bfloat16)
    ffn_ref[...] = ffn_in
    mix_ref[...] = jnp.where(core == 0, after_wide[:half], after_wide[half:]).astype(jnp.bfloat16)
    slots = taken_ref.shape[0]
    slot = lax.broadcasted_iota(jnp.int32, (slots, rows), 0)
    expert = slot // 2 * 2 + core
    named = jnp.zeros((slots, rows), jnp.float32)
    for n in range(routes_ref.shape[0]):
        named = jnp.where(routes_ref[n : n + 1, :] == expert, 1.0, named)
    earlier = jnp.where(
        lax.broadcasted_iota(jnp.int32, (rows, rows), 0)
        < lax.broadcasted_iota(jnp.int32, (rows, rows), 1),
        1.0,
        0.0,
    ).astype(jnp.bfloat16)
    before = jnp.dot(named.astype(jnp.bfloat16), earlier, preferred_element_type=jnp.float32)
    taken = jnp.where(before == (slot % 2).astype(jnp.float32), named, 0.0).astype(jnp.bfloat16)
    taken_ref[...] = taken
    outgoing = jnp.dot(taken, ffn_in, preferred_element_type=jnp.float32).astype(jnp.bfloat16)
    outgoing_ref[...] = outgoing.reshape(outgoing_ref.shape)


def spread(place, own_pieces, other_pieces, own_hidden, other_hidden, gain_mix, gain_in, routes, slots):
    rows, width = 2 * own_hidden.shape[0], own_hidden.shape[1]
    return pl.pallas_call(
        spread_kernel,
        in_specs=[pl.BlockSpec(memory_space=pltpu.SMEM)]
        + [pl.BlockSpec(memory_space=pltpu.VMEM)] * 7,
        out_specs=[pl.BlockSpec(memory_space=pltpu.VMEM)] * 4,
        out_shape=[
            jax.ShapeDtypeStruct((slots // 2, 2, width), jnp.bfloat16),
            jax.ShapeDtypeStruct((rows, width), jnp.bfloat16),
            jax.ShapeDtypeStruct((rows // 2, width), jnp.bfloat16),
            jax.ShapeDtypeStruct((slots, rows), jnp.bfloat16),
        ],
        compiler_params=pltpu.CompilerParams(vmem_limit_bytes=8 << 20),
        name="spread",
    )(
        place,
        own_pieces,
        other_pieces,
        own_hidden,
        other_hidden,
        gain_mix,
        gain_in,
        routes.T,
    )


def experts_kernel(rows_ref, gate_ref, up_ref, down_ref, out_ref):
    rows = rows_ref[...].reshape(-1, rows_ref.shape[-1])
    gate_part = jnp.dot(rows, gate_ref[...], preferred_element_type=jnp.float32)
    up_part = jnp.dot(rows, up_ref[...], preferred_element_type=jnp.float32)
    inner = (gate_part / (1.0 + jnp.exp(-gate_part)) * up_part).astype(jnp.bfloat16)
    out = jnp.dot(inner, down_ref[...], preferred_element_type=jnp.float32)
    out_ref[...] = out.astype(out_ref.dtype).reshape(out_ref.shape)


def expert_rows(rows, gate_w, up_w, down_w):
    return pl.pallas_call(
        experts_kernel,
        in_specs=[pl.BlockSpec(memory_space=pltpu.VMEM)] * 4,
        out_specs=pl.BlockSpec(memory_space=pltpu.VMEM),
        out_shape=jax.ShapeDtypeStruct(rows.shape, jnp.bfloat16),
        compiler_params=pltpu.CompilerParams(vmem_limit_bytes=10 << 20),
    )(rows, gate_w, up_w, down_w)


def gathered_kernel(place_ref, weights_ref, returned_ref, shared_ref, kept_ref, given_ref):
    core = place_ref[0]
    rows = weights_ref.shape[0] // 2
    half = rows // 2
    returned = returned_ref[...].reshape(-1, returned_ref.shape[-1])
    both = jnp.dot(weights_ref[...], returned, preferred_element_type=jnp.float32)
    routed = both[:rows] + both[rows:]
    first, second = routed[:half], routed[half:]
    shared = shared_ref[...].astype(jnp.float32)
    kept_ref[...] = jnp.where(core == 0, first, second) + shared
    given_ref[...] = jnp.where(core == 0, second, first)


def gathered(place, weights, returned, shared):
    shape = jax.ShapeDtypeStruct(shared.shape, jnp.float32)
    return pl.pallas_call(
        gathered_kernel,
        in_specs=[pl.BlockSpec(memory_space=pltpu.SMEM)]
        + [pl.BlockSpec(memory_space=pltpu.VMEM)] * 3,
        out_specs=[pl.BlockSpec(memory_space=pltpu.VMEM)] * 2,
        out_shape=[shape, shape],
        compiler_params=pltpu.CompilerParams(vmem_limit_bytes=8 << 20),
        name="gathered",
    )(place, weights, returned, shared)


def routed_kernel(
    rows_hbm,
    gate_hbm,
    up_hbm,
    down_hbm,
    out_hbm,
    rows_ref,
    gate_ref,
    up_ref,
    down_ref,
    out_ref,
    arrived,
    left,
):
    moves = [
        pltpu.make_async_copy(source, target, arrived.at[n])
        for n, (source, target) in enumerate(
            (
                (rows_hbm, rows_ref),
                (gate_hbm, gate_ref),
                (up_hbm, up_ref),
                (down_hbm, down_ref),
            )
        )
    ]
    for move in moves:
        move.start()
    moves[0].wait()
    rows = rows_ref[...].reshape(-1, rows_ref.shape[-1])
    moves[1].wait()
    gate_part = jnp.dot(rows, gate_ref[...], preferred_element_type=jnp.float32)
    moves[2].wait()
    up_part = jnp.dot(rows, up_ref[...], preferred_element_type=jnp.float32)
    inner = (gate_part / (1.0 + jnp.exp(-gate_part)) * up_part).astype(jnp.bfloat16)
    moves[3].wait()
    chunk = out_ref.shape[-1] // OUT_CHUNKS
    sent = []
    for n in range(OUT_CHUNKS):
        columns = pl.ds(n * chunk, chunk)
        out = jnp.dot(inner, down_ref[:, columns], preferred_element_type=jnp.float32)
        out_ref[:, :, columns] = out.astype(out_ref.dtype).reshape(*out_ref.shape[:2], chunk)
        sent.append(
            pltpu.make_async_copy(
                out_ref.at[:, :, columns], out_hbm.at[:, :, columns], left.at[n]
            )
        )
        sent[-1].start()
    for move in sent:
        move.wait()


def routed_rows(rows, gate_w, up_w, down_w):
    return pl.pallas_call(
        routed_kernel,
        in_specs=[pl.BlockSpec(memory_space=pltpu.HBM)] * 4,
        out_specs=pl.BlockSpec(memory_space=pltpu.HBM),
        out_shape=jax.ShapeDtypeStruct(rows.shape, jnp.bfloat16),
        scratch_shapes=[pltpu.VMEM(w.shape, w.dtype) for w in (rows, gate_w, up_w, down_w, rows)]
        + [pltpu.SemaphoreType.DMA((4,)), pltpu.SemaphoreType.DMA((OUT_CHUNKS,))],
        compiler_params=pltpu.CompilerParams(vmem_limit_bytes=64300 << 10),
        name="routed",
    )(rows, gate_w, up_w, down_w)


def local(
    hidden_in,
    query_nope,
    query_rope,
    new_latent,
    new_rope,
    cache_latent,
    cache_rope,
    lengths,
    absorb_key,
    value_up,
    out_proj,
    gain_mix,
    gain_ffn_in,
    router,
    routes,
    expert_gate,
    expert_up,
    expert_down,
    shared_gate,
    shared_up,
    shared_down,
    gain_ffn_out,
):
    seq_count, _ = hidden_in.shape
    core = lax.axis_index("tp")
    own_start = core * seq_count
    place = core[None].astype(jnp.int32)
    halves = in_parts(out_proj.T, HALVES, len(COLUMN_GROUPS[0]) // HALVES)
    slab = exchanged(halves, COLUMN_GROUPS).reshape(-1, halves.shape[-1])
    other_slab = from_other_core(slab)
    other_hidden = from_other_core(hidden_in)
    heads_out = attention(
        query_nope,
        query_rope,
        new_latent,
        new_rope,
        cache_latent,
        cache_rope,
        lengths,
        absorb_key,
        value_up,
    )
    block_heads = exchanged(in_parts(heads_out, HALVES, len(BLOCKS[0]) // HALVES), BLOCKS)
    block_heads, other_hidden = lax.optimization_barrier((block_heads, other_hidden))
    partial = projected(place, block_heads, slab, other_slab)
    pieces = exchanged(partial, BLOCKS)
    other_pieces = from_other_core(pieces)
    experts_total = router.shape[1]
    group_rows, top_count = routes.shape
    ep_count = lax.axis_size(EP)
    capacity = 2 * ((group_rows * top_count + experts_total - 1) // experts_total)
    slots = ep_count * capacity
    slot_expert = lax.iota(jnp.int32, slots) // capacity * 2 + core
    outgoing, ffn_in, own_mix, taken = spread(
        place,
        pieces,
        other_pieces,
        hidden_in,
        other_hidden,
        gain_mix,
        gain_ffn_in,
        routes,
        slots,
    )
    received = lax.all_to_all(
        outgoing, EP, split_axis=0, concat_axis=0, tiled=True
    )
    affinity = jax.nn.sigmoid(jnp.dot(ffn_in, router, preferred_element_type=jnp.float32))
    choose = routes[..., None] == lax.iota(jnp.int32, experts_total)[None, None, :]
    chosen = jnp.sum(jnp.where(choose, affinity[:, None, :], 0.0), axis=-1)
    route_weights = chosen / jnp.sum(chosen, axis=-1, keepdims=True) * routed_scale
    slot_weights = jnp.sum(
        jnp.where(
            routes[:, :, None] == slot_expert[None, None, :], route_weights[:, :, None], 0.0
        ),
        axis=1,
    )
    slot_weights = slot_weights * taken.T.astype(jnp.float32)
    weights_high = slot_weights.astype(jnp.bfloat16)
    weights_low = (slot_weights - weights_high.astype(jnp.float32)).astype(jnp.bfloat16)
    own_ffn = lax.dynamic_slice_in_dim(ffn_in, own_start, seq_count, 0)
    shared = expert_rows(own_ffn, shared_gate, shared_up, shared_down)
    outputs = routed_rows(received, expert_gate[0], expert_up[0], expert_down[0])
    returned = lax.all_to_all(outputs, EP, split_axis=0, concat_axis=0, tiled=True)
    weights = jnp.concatenate([weights_high, weights_low], axis=0)
    kept, given = gathered(place, weights, returned, shared)
    combined = kept + from_other_core(given)
    return (
        own_mix.astype(jnp.float32) + gain_ffn_out.astype(jnp.float32) * normalize(combined)
    ).astype(jnp.bfloat16)


def solution(mesh):
    torus = Mesh(
        mesh.devices.reshape(mesh.shape["grp"], 8, 8, mesh.shape["tp"]),
        ("grp", "ep_0", "ep_1", "tp"),
    )
    in_specs = (
        P(GRP_EP_TP, None),
        P(GRP_EP_TP, None, None),
        P(GRP_EP_TP, None, None),
        P(GRP_EP_TP, None),
        P(GRP_EP_TP, None),
        P(GRP_EP_TP, None, None),
        P(GRP_EP_TP, None, None),
        P(GRP_EP_TP),
        P(),
        P(),
        P(None, EP_TP),
        P(),
        P(),
        P(),
        P(GRP_EP, None),
        P(EP_TP, None, None),
        P(EP_TP, None, None),
        P(EP_TP, None, None),
        P(),
        P(),
        P(),
        P(),
    )
    out_specs = P(GRP_EP_TP, None)

    return jax.shard_map(local, mesh=torus, in_specs=in_specs, out_specs=out_specs, check_vma=False)
```

```python
import math

import jax
import jax.numpy as jnp
from jax import lax
from jax.experimental import pallas as pl
from jax.experimental.pallas import tpu as pltpu
from jax.sharding import Mesh
from jax.sharding import PartitionSpec as P

SEQ_STEP = 4
OUT_CHUNKS = 4
EP = ("ep_0", "ep_1")
GRP_EP_TP = ("grp", "ep_0", "ep_1", "tp")
EP_TP = ("ep_0", "ep_1", "tp")
GRP_EP = ("grp", "ep_0", "ep_1")


rope_theta = 10000.0
norm_eps = 1e-06
routed_scale = 2.5
masked_score = -1e30


def device_at(row, col, core):
    return (row * 8 + col) * 2 + core


COLUMN_GROUPS = [
    [device_at(row, col, core) for col in range(8)] for row in range(8) for core in range(2)
]
BLOCKS = [
    [device_at(row, 2 * pair + col, core) for row in range(8) for col in range(2)]
    for pair in range(4)
    for core in range(2)
]
HALVES = 2


def repeat_kernel(array_ref, out_ref):
    run = out_ref.shape[-1]
    count = array_ref.shape[-1] // run
    for n in range(out_ref.shape[0]):
        out_ref[n] = array_ref[:, n % count * run : (n % count + 1) * run]


def in_parts(array, count, times):
    rows, width = array.shape
    return pl.pallas_call(
        repeat_kernel,
        in_specs=[pl.BlockSpec(memory_space=pltpu.VMEM)],
        out_specs=pl.BlockSpec(memory_space=pltpu.VMEM),
        out_shape=jax.ShapeDtypeStruct((count * times, rows, width // count), array.dtype),
        compiler_params=pltpu.CompilerParams(vmem_limit_bytes=4 << 20),
        name="parts",
    )(array)


def project_kernel(place_ref, heads_ref, own_slab_ref, other_slab_ref, out_ref):
    core = place_ref[0]
    heads = heads_ref[...].reshape(-1, heads_ref.shape[-1])
    dims = (((1,), (1,)), ((), ()))
    own = lax.dot_general(heads, own_slab_ref[...], dims, preferred_element_type=jnp.float32)
    other = lax.dot_general(heads, other_slab_ref[...], dims, preferred_element_type=jnp.float32)
    joined = jnp.concatenate(
        [jnp.where(core == 0, own, other), jnp.where(core == 0, other, own)], axis=-1
    ).astype(jnp.bfloat16)
    count = joined.shape[-1]
    source = lax.broadcasted_iota(jnp.int32, (count, count), 0)
    target = lax.broadcasted_iota(jnp.int32, (count, count), 1)
    run = count // 16
    goes_to = source % (count // 2) // run * (2 * run) + source // (count // 2) * run + source % run
    order = jnp.where(goes_to == target, 1.0, 0.0).astype(jnp.bfloat16)
    out = jnp.dot(joined, order, preferred_element_type=jnp.float32)
    out_ref[...] = out.astype(jnp.bfloat16).reshape(out_ref.shape)


def projected(place, heads, own_slab, other_slab):
    return pl.pallas_call(
        project_kernel,
        in_specs=[pl.BlockSpec(memory_space=pltpu.SMEM)]
        + [pl.BlockSpec(memory_space=pltpu.VMEM)] * 3,
        out_specs=pl.BlockSpec(memory_space=pltpu.VMEM),
        out_shape=jax.ShapeDtypeStruct((*heads.shape[:2], 2 * own_slab.shape[0]), jnp.bfloat16),
        compiler_params=pltpu.CompilerParams(vmem_limit_bytes=6 << 20),
        name="projected",
    )(place, heads, own_slab, other_slab)


def exchanged(blocks, groups):
    return lax.all_to_all(blocks, EP_TP, 0, 0, axis_index_groups=groups, tiled=True)


def from_other_core(array):
    return lax.ppermute(array, "tp", [(0, 1), (1, 0)])


def normalize(values):
    return values * lax.rsqrt(jnp.mean(values * values, axis=-1, keepdims=True) + norm_eps)


def attention_kernel(
    lengths_ref,
    nope_ref,
    rope_ref,
    latent_ref,
    key_ref,
    absorb_ref,
    cache_hbm,
    cache_rope_hbm,
    out_ref,
    cache_ref,
    cache_rope_ref,
    arrived,
):
    moves = []
    for n in range(cache_ref.shape[0] // SEQ_STEP):
        group = pl.ds(n * SEQ_STEP, SEQ_STEP)
        moves.append(
            (
                pltpu.make_async_copy(cache_hbm.at[group], cache_ref.at[group], arrived.at[n, 0]),
                pltpu.make_async_copy(
                    cache_rope_hbm.at[group], cache_rope_ref.at[group], arrived.at[n, 1]
                ),
            )
        )
    for pair in moves:
        for move in pair:
            move.start()
    seq_count, heads, nope = nope_ref.shape
    rope = rope_ref.shape[-1]
    half = rope // 2
    latent = cache_ref.shape[-1]
    scale = (nope + rope) ** (-0.5)

    def turned(values, cosine, sine):
        swapped = jnp.concatenate([values[..., half:], values[..., :half]], axis=-1)
        return values * cosine + swapped * sine

    rows = nope_ref[...].reshape(seq_count * heads, nope)
    twice = jnp.concatenate([rows, rows], axis=-1)
    wide = jnp.concatenate([twice] * (heads // 2), axis=-1)
    row_head = lax.broadcasted_iota(jnp.int32, wide.shape, 0) % heads
    column_head = lax.broadcasted_iota(jnp.int32, wide.shape, 1) // nope
    wide = jnp.where(row_head == column_head, wide.astype(jnp.float32), 0.0)
    queries = jnp.dot(
        wide.astype(jnp.bfloat16), absorb_ref[...], preferred_element_type=jnp.float32
    )
    query_all = queries.reshape(seq_count, heads, latent).astype(jnp.bfloat16)
    row = lax.broadcasted_iota(jnp.int32, (seq_count, rope), 0)
    column = lax.broadcasted_iota(jnp.int32, (seq_count, rope), 1)
    position = jnp.zeros((seq_count, rope), jnp.int32)
    for n in range(seq_count):
        position = jnp.where(row == n, lengths_ref[n], position)
    exponent = (column % half).astype(jnp.float32) * (-2.0 / rope * math.log(rope_theta))
    angles = position.astype(jnp.float32) * jnp.exp(exponent)
    cosine = jnp.cos(angles)
    sine = jnp.sin(angles)
    sine = jnp.where(column < half, -sine, sine)
    query_pe_all = turned(
        rope_ref[...].astype(jnp.float32), cosine[:, None, :], sine[:, None, :]
    ).astype(jnp.bfloat16)
    latent_new = normalize(latent_ref[...].astype(jnp.float32)).astype(jnp.bfloat16)
    latent_new_all = latent_new.astype(jnp.float32)[:, None, :]
    key_new = turned(key_ref[...].astype(jnp.float32), cosine, sine)
    key_new_all = key_new.astype(jnp.bfloat16).astype(jnp.float32)[:, None, :]

    for step in range(len(moves)):
        places = range(SEQ_STEP)
        seqs = [step * SEQ_STEP + place for place in places]
        rows = SEQ_STEP * heads
        group = slice(step * SEQ_STEP, (step + 1) * SEQ_STEP)
        query = query_all[group]
        query_pe = query_pe_all[group]
        latent_wide = latent_new_all[group]
        key_wide = key_new_all[group]
        for move in moves[step]:
            move.wait()
        score_new = (
            jnp.sum(query.astype(jnp.float32) * latent_wide, axis=-1, keepdims=True)
            + jnp.sum(query_pe.astype(jnp.float32) * key_wide, axis=-1, keepdims=True)
        ).reshape(rows, 1) * scale
        parts = [
            lax.dot_general(
                query[place], cache_ref[seqs[place]], (((1,), (1,)), ((), ())),
                preferred_element_type=jnp.float32,
            )
            + jnp.dot(query_pe[place], cache_rope_ref[seqs[place]], preferred_element_type=jnp.float32)
            for place in places
        ]
        position = lax.broadcasted_iota(jnp.int32, parts[0].shape, 1)
        scores = jnp.concatenate(
            [
                jnp.where(position < lengths_ref[seq], part * scale, masked_score)
                for seq, part in zip(seqs, parts)
            ],
            axis=0,
        )
        row_max = jnp.maximum(jnp.max(scores, axis=-1, keepdims=True), score_new)
        weights = jnp.exp(scores - row_max)
        weight_new = jnp.exp(score_new - row_max)
        total = jnp.sum(weights, axis=-1, keepdims=True) + weight_new
        rounded = weights.astype(jnp.bfloat16)
        summed = jnp.concatenate(
            [
                jnp.dot(
                    rounded[place * heads : (place + 1) * heads],
                    cache_ref[seqs[place]],
                    preferred_element_type=jnp.float32,
                )
                for place in places
            ],
            axis=0,
        )
        fresh = jnp.broadcast_to(latent_wide, query.shape).reshape(rows, latent)
        summed = summed + weight_new.astype(jnp.bfloat16).astype(jnp.float32) * fresh
        out_ref[group] = (summed / total).astype(jnp.bfloat16).reshape(SEQ_STEP, heads, latent)


def attended(query_nope, query_rope, new_latent, new_rope, cache_latent, cache_rope, lengths, absorb_key):
    seq_count, heads, nope = query_nope.shape
    rope = query_rope.shape[-1]
    latent = cache_latent.shape[-1]
    context = cache_latent.shape[1]
    absorb = absorb_key.transpose(1, 2, 0).reshape(heads * nope, latent)
    rope_turned = cache_rope.transpose(0, 2, 1)
    return pl.pallas_call(
        attention_kernel,
        in_specs=[pl.BlockSpec(memory_space=pltpu.SMEM)]
        + [pl.BlockSpec(memory_space=pltpu.VMEM)] * 5
        + [pl.BlockSpec(memory_space=pltpu.HBM)] * 2,
        out_specs=pl.BlockSpec(memory_space=pltpu.VMEM),
        scratch_shapes=[
            pltpu.VMEM(cache_latent.shape, jnp.bfloat16),
            pltpu.VMEM(rope_turned.shape, jnp.bfloat16),
            pltpu.SemaphoreType.DMA((seq_count // SEQ_STEP, 2)),
        ],
        out_shape=jax.ShapeDtypeStruct((seq_count, heads, latent), jnp.bfloat16),
        compiler_params=pltpu.CompilerParams(vmem_limit_bytes=60 * 1024 * 1024),
        cost_estimate=pl.CostEstimate(
            flops=8 * seq_count * heads * context * latent,
            bytes_accessed=2 * seq_count * context * (latent + rope),
            transcendentals=seq_count * heads * context,
        ),
        name="attended",
    )(
        lengths, query_nope, query_rope, new_latent, new_rope, absorb, cache_latent, rope_turned
    )


def attention(
    query_nope,
    query_rope,
    new_latent,
    new_rope,
    cache_latent,
    cache_rope,
    lengths,
    absorb_key,
    value_up,
):
    latent_out = attended(
        query_nope, query_rope, new_latent, new_rope, cache_latent, cache_rope, lengths, absorb_key
    )
    return (
        jnp.einsum("shc,chv->shv", latent_out, value_up, preferred_element_type=jnp.float32)
        .astype(jnp.bfloat16)
        .reshape(latent_out.shape[0], -1)
    )


def spread_kernel(
    place_ref,
    own_pieces_ref,
    other_pieces_ref,
    own_hidden_ref,
    other_hidden_ref,
    gain_mix_ref,
    gain_in_ref,
    routes_ref,
    outgoing_ref,
    ffn_ref,
    mix_ref,
    taken_ref,
):
    core = place_ref[0]
    half = own_hidden_ref.shape[0]
    rows = 2 * half

    def in_columns(pieces_ref):
        parts = [
            pieces_ref[HALVES * n].astype(jnp.float32) + pieces_ref[HALVES * n + 1].astype(jnp.float32)
            for n in range(pieces_ref.shape[0] // HALVES)
        ]
        return jnp.concatenate(parts, axis=-1)

    own_mixed = in_columns(own_pieces_ref)
    other_mixed = in_columns(other_pieces_ref)
    mixed = jnp.concatenate(
        [
            jnp.where(core == 0, own_mixed, other_mixed),
            jnp.where(core == 0, other_mixed, own_mixed),
        ],
        axis=0,
    )
    mixed = mixed.astype(jnp.bfloat16).astype(jnp.float32)
    own_hidden = own_hidden_ref[...].astype(jnp.float32)
    other_hidden = other_hidden_ref[...].astype(jnp.float32)
    hidden = jnp.concatenate(
        [
            jnp.where(core == 0, own_hidden, other_hidden),
            jnp.where(core == 0, other_hidden, own_hidden),
        ],
        axis=0,
    )
    after_mix = (
        hidden
        + gain_mix_ref[...].astype(jnp.float32)[None] * normalize(mixed)
    ).astype(jnp.bfloat16)
    after_wide = after_mix.astype(jnp.float32)
    ffn_in = (normalize(after_wide) * gain_in_ref[...].astype(jnp.float32)[None]).astype(jnp.bfloat16)
    ffn_ref[...] = ffn_in
    mix_ref[...] = jnp.where(core == 0, after_wide[:half], after_wide[half:]).astype(jnp.bfloat16)
    slots = taken_ref.shape[0]
    slot = lax.broadcasted_iota(jnp.int32, (slots, rows), 0)
    expert = slot // 2 * 2 + core
    named = jnp.zeros((slots, rows), jnp.float32)
    for n in range(routes_ref.shape[0]):
        named = jnp.where(routes_ref[n : n + 1, :] == expert, 1.0, named)
    earlier = jnp.where(
        lax.broadcasted_iota(jnp.int32, (rows, rows), 0)
        < lax.broadcasted_iota(jnp.int32, (rows, rows), 1),
        1.0,
        0.0,
    ).astype(jnp.bfloat16)
    before = jnp.dot(named.astype(jnp.bfloat16), earlier, preferred_element_type=jnp.float32)
    taken = jnp.where(before == (slot % 2).astype(jnp.float32), named, 0.0).astype(jnp.bfloat16)
    taken_ref[...] = taken
    outgoing = jnp.dot(taken, ffn_in, preferred_element_type=jnp.float32).astype(jnp.bfloat16)
    outgoing_ref[...] = outgoing.reshape(outgoing_ref.shape)


def spread(place, own_pieces, other_pieces, own_hidden, other_hidden, gain_mix, gain_in, routes, slots):
    rows, width = 2 * own_hidden.shape[0], own_hidden.shape[1]
    return pl.pallas_call(
        spread_kernel,
        in_specs=[pl.BlockSpec(memory_space=pltpu.SMEM)]
        + [pl.BlockSpec(memory_space=pltpu.VMEM)] * 7,
        out_specs=[pl.BlockSpec(memory_space=pltpu.VMEM)] * 4,
        out_shape=[
            jax.ShapeDtypeStruct((slots // 2, 2, width), jnp.bfloat16),
            jax.ShapeDtypeStruct((rows, width), jnp.bfloat16),
            jax.ShapeDtypeStruct((rows // 2, width), jnp.bfloat16),
            jax.ShapeDtypeStruct((slots, rows), jnp.bfloat16),
        ],
        compiler_params=pltpu.CompilerParams(vmem_limit_bytes=8 << 20),
        name="spread",
    )(
        place,
        own_pieces,
        other_pieces,
        own_hidden,
        other_hidden,
        gain_mix,
        gain_in,
        routes.T,
    )


def experts_kernel(rows_ref, gate_ref, up_ref, down_ref, out_ref):
    rows = rows_ref[...].reshape(-1, rows_ref.shape[-1])
    gate_part = jnp.dot(rows, gate_ref[...], preferred_element_type=jnp.float32)
    up_part = jnp.dot(rows, up_ref[...], preferred_element_type=jnp.float32)
    inner = (gate_part / (1.0 + jnp.exp(-gate_part)) * up_part).astype(jnp.bfloat16)
    out = jnp.dot(inner, down_ref[...], preferred_element_type=jnp.float32)
    out_ref[...] = out.astype(out_ref.dtype).reshape(out_ref.shape)


def expert_rows(rows, gate_w, up_w, down_w):
    return pl.pallas_call(
        experts_kernel,
        in_specs=[pl.BlockSpec(memory_space=pltpu.VMEM)] * 4,
        out_specs=pl.BlockSpec(memory_space=pltpu.VMEM),
        out_shape=jax.ShapeDtypeStruct(rows.shape, jnp.bfloat16),
        compiler_params=pltpu.CompilerParams(vmem_limit_bytes=10 << 20),
    )(rows, gate_w, up_w, down_w)


def gathered_kernel(place_ref, weights_ref, returned_ref, shared_ref, kept_ref, given_ref):
    core = place_ref[0]
    rows = weights_ref.shape[0] // 2
    half = rows // 2
    returned = returned_ref[...].reshape(-1, returned_ref.shape[-1])
    both = jnp.dot(weights_ref[...], returned, preferred_element_type=jnp.float32)
    routed = both[:rows] + both[rows:]
    first, second = routed[:half], routed[half:]
    shared = shared_ref[...].astype(jnp.float32)
    kept_ref[...] = jnp.where(core == 0, first, second) + shared
    given_ref[...] = jnp.where(core == 0, second, first)


def gathered(place, weights, returned, shared):
    shape = jax.ShapeDtypeStruct(shared.shape, jnp.float32)
    return pl.pallas_call(
        gathered_kernel,
        in_specs=[pl.BlockSpec(memory_space=pltpu.SMEM)]
        + [pl.BlockSpec(memory_space=pltpu.VMEM)] * 3,
        out_specs=[pl.BlockSpec(memory_space=pltpu.VMEM)] * 2,
        out_shape=[shape, shape],
        compiler_params=pltpu.CompilerParams(vmem_limit_bytes=8 << 20),
        name="gathered",
    )(place, weights, returned, shared)


def routed_kernel(
    rows_hbm,
    gate_hbm,
    up_hbm,
    down_hbm,
    out_hbm,
    rows_ref,
    gate_ref,
    up_ref,
    down_ref,
    out_ref,
    arrived,
    left,
):
    moves = [
        pltpu.make_async_copy(source, target, arrived.at[n])
        for n, (source, target) in enumerate(
            (
                (rows_hbm, rows_ref),
                (gate_hbm, gate_ref),
                (up_hbm, up_ref),
                (down_hbm, down_ref),
            )
        )
    ]
    for move in moves:
        move.start()
    moves[0].wait()
    rows = rows_ref[...].reshape(-1, rows_ref.shape[-1])
    moves[1].wait()
    gate_part = jnp.dot(rows, gate_ref[...], preferred_element_type=jnp.float32)
    moves[2].wait()
    up_part = jnp.dot(rows, up_ref[...], preferred_element_type=jnp.float32)
    inner = (gate_part / (1.0 + jnp.exp(-gate_part)) * up_part).astype(jnp.bfloat16)
    moves[3].wait()
    chunk = out_ref.shape[-1] // OUT_CHUNKS
    sent = []
    for n in range(OUT_CHUNKS):
        columns = pl.ds(n * chunk, chunk)
        out = jnp.dot(inner, down_ref[:, columns], preferred_element_type=jnp.float32)
        out_ref[:, :, columns] = out.astype(out_ref.dtype).reshape(*out_ref.shape[:2], chunk)
        sent.append(
            pltpu.make_async_copy(
                out_ref.at[:, :, columns], out_hbm.at[:, :, columns], left.at[n]
            )
        )
        sent[-1].start()
    for move in sent:
        move.wait()


def routed_rows(rows, gate_w, up_w, down_w):
    return pl.pallas_call(
        routed_kernel,
        in_specs=[pl.BlockSpec(memory_space=pltpu.HBM)] * 4,
        out_specs=pl.BlockSpec(memory_space=pltpu.HBM),
        out_shape=jax.ShapeDtypeStruct(rows.shape, jnp.bfloat16),
        scratch_shapes=[pltpu.VMEM(w.shape, w.dtype) for w in (rows, gate_w, up_w, down_w, rows)]
        + [pltpu.SemaphoreType.DMA((4,)), pltpu.SemaphoreType.DMA((OUT_CHUNKS,))],
        compiler_params=pltpu.CompilerParams(vmem_limit_bytes=64300 << 10),
        name="routed",
    )(rows, gate_w, up_w, down_w)


def close_kernel(kept_ref, other_ref, mix_ref, gain_ref, out_ref):
    combined = kept_ref[...] + other_ref[...]
    out_ref[...] = (
        mix_ref[...].astype(jnp.float32)
        + gain_ref[...].astype(jnp.float32)[None] * normalize(combined)
    ).astype(jnp.bfloat16)


def closed(kept, other, own_mix, gain):
    return pl.pallas_call(
        close_kernel,
        in_specs=[pl.BlockSpec(memory_space=pltpu.VMEM)] * 4,
        out_specs=pl.BlockSpec(memory_space=pltpu.VMEM),
        out_shape=jax.ShapeDtypeStruct(kept.shape, jnp.bfloat16),
        compiler_params=pltpu.CompilerParams(vmem_limit_bytes=4 << 20),
        name="closed",
    )(kept, other, own_mix, gain)


def local(
    hidden_in,
    query_nope,
    query_rope,
    new_latent,
    new_rope,
    cache_latent,
    cache_rope,
    lengths,
    absorb_key,
    value_up,
    out_proj,
    gain_mix,
    gain_ffn_in,
    router,
    routes,
    expert_gate,
    expert_up,
    expert_down,
    shared_gate,
    shared_up,
    shared_down,
    gain_ffn_out,
):
    seq_count, _ = hidden_in.shape
    core = lax.axis_index("tp")
    own_start = core * seq_count
    place = core[None].astype(jnp.int32)
    halves = in_parts(out_proj.T, HALVES, len(COLUMN_GROUPS[0]) // HALVES)
    slab = exchanged(halves, COLUMN_GROUPS).reshape(-1, halves.shape[-1])
    other_slab = from_other_core(slab)
    other_hidden = from_other_core(hidden_in)
    heads_out = attention(
        query_nope,
        query_rope,
        new_latent,
        new_rope,
        cache_latent,
        cache_rope,
        lengths,
        absorb_key,
        value_up,
    )
    block_heads = exchanged(in_parts(heads_out, HALVES, len(BLOCKS[0]) // HALVES), BLOCKS)
    block_heads, other_hidden = lax.optimization_barrier((block_heads, other_hidden))
    partial = projected(place, block_heads, slab, other_slab)
    pieces = exchanged(partial, BLOCKS)
    other_pieces = from_other_core(pieces)
    experts_total = router.shape[1]
    group_rows, top_count = routes.shape
    ep_count = lax.axis_size(EP)
    capacity = 2 * ((group_rows * top_count + experts_total - 1) // experts_total)
    slots = ep_count * capacity
    slot_expert = lax.iota(jnp.int32, slots) // capacity * 2 + core
    outgoing, ffn_in, own_mix, taken = spread(
        place,
        pieces,
        other_pieces,
        hidden_in,
        other_hidden,
        gain_mix,
        gain_ffn_in,
        routes,
        slots,
    )
    received = lax.all_to_all(
        outgoing, EP, split_axis=0, concat_axis=0, tiled=True
    )
    affinity = jax.nn.sigmoid(jnp.dot(ffn_in, router, preferred_element_type=jnp.float32))
    choose = routes[..., None] == lax.iota(jnp.int32, experts_total)[None, None, :]
    chosen = jnp.sum(jnp.where(choose, affinity[:, None, :], 0.0), axis=-1)
    route_weights = chosen / jnp.sum(chosen, axis=-1, keepdims=True) * routed_scale
    slot_weights = jnp.sum(
        jnp.where(
            routes[:, :, None] == slot_expert[None, None, :], route_weights[:, :, None], 0.0
        ),
        axis=1,
    )
    slot_weights = slot_weights * taken.T.astype(jnp.float32)
    weights_high = slot_weights.astype(jnp.bfloat16)
    weights_low = (slot_weights - weights_high.astype(jnp.float32)).astype(jnp.bfloat16)
    own_ffn = lax.dynamic_slice_in_dim(ffn_in, own_start, seq_count, 0)
    shared = expert_rows(own_ffn, shared_gate, shared_up, shared_down)
    outputs = routed_rows(received, expert_gate[0], expert_up[0], expert_down[0])
    returned = lax.all_to_all(outputs, EP, split_axis=0, concat_axis=0, tiled=True)
    weights = jnp.concatenate([weights_high, weights_low], axis=0)
    kept, given = gathered(place, weights, returned, shared)
    return closed(kept, from_other_core(given), own_mix, gain_ffn_out)


def solution(mesh):
    torus = Mesh(
        mesh.devices.reshape(mesh.shape["grp"], 8, 8, mesh.shape["tp"]),
        ("grp", "ep_0", "ep_1", "tp"),
    )
    in_specs = (
        P(GRP_EP_TP, None),
        P(GRP_EP_TP, None, None),
        P(GRP_EP_TP, None, None),
        P(GRP_EP_TP, None),
        P(GRP_EP_TP, None),
        P(GRP_EP_TP, None, None),
        P(GRP_EP_TP, None, None),
        P(GRP_EP_TP),
        P(),
        P(),
        P(None, EP_TP),
        P(),
        P(),
        P(),
        P(GRP_EP, None),
        P(EP_TP, None, None),
        P(EP_TP, None, None),
        P(EP_TP, None, None),
        P(),
        P(),
        P(),
        P(),
    )
    out_specs = P(GRP_EP_TP, None)

    return jax.shard_map(local, mesh=torus, in_specs=in_specs, out_specs=out_specs, check_vma=False)
```
